256 devices in a mesh: kv: 32 (over z, y), tp: 8 (over x, core).
Axes of the slice: x: 4, y: 4, z: 8, core: 2. Of those that a mesh axis runs over, the one named last changes fastest.
Arguments:
- piece_tokens: bfloat16 [3072, 4096], P('kv'), may hold values from -6 to 6
- step_tokens: bfloat16 [32, 4096], P('kv'), may hold values from -6 to 6
- in_gain: float32 [4096], replicated, may hold values from 0.1 to 1.9
- w_query: bfloat16 [4096, 8, 2, 128], P(None, 'tp'), may hold values from -0.09375 to 0.09375
- w_key: bfloat16 [4096, 8, 2, 128], P(None, 'tp'), may hold values from -0.15625 to 0.15625
- w_value: bfloat16 [4096, 8, 256], P(None, 'tp'), may hold values from -0.09375 to 0.09375
- w_out: bfloat16 [8, 256, 4096], P('tp'), may hold values from -0.125 to 0.125
- mix_ratio: float32 [8], P('tp'), may hold values from 0.3 to 0.8
- out_gain: float32 [256], replicated, may hold values from 0.1 to 1.9
- prompt_keys: bfloat16 [65536, 8, 2, 128], P('kv', 'tp'), may hold values from -630 to 630
- prompt_values: bfloat16 [65536, 8, 256], P('kv', 'tp'), may hold values from -6 to 6
- step_cache_keys: bfloat16 [32, 4096, 8, 2, 128], P(None, 'kv', 'tp'), may hold values from -630 to 630
- step_cache_values: bfloat16 [32, 4096, 8, 256], P(None, 'kv', 'tp'), may hold values from -6 to 6
- prompt_len: int32 [1], replicated, may hold values from 64512 to 65536
- step_lens: int32 [32], replicated, may hold values from 4032 to 4096
Outputs:
- piece_out: bfloat16 [3072, 4096], P('kv', 'tp')
- step_out: bfloat16 [32, 4096], P('kv', 'tp')
- piece_keys: bfloat16 [3072, 8, 2, 128], P('kv', 'tp')
- piece_values: bfloat16 [3072, 8, 256], P('kv', 'tp')
- step_keys: bfloat16 [32, 8, 2, 128], P('kv', 'tp')
- step_values: bfloat16 [32, 8, 256], P('kv', 'tp')
The draws below stay inside these ranges and needn't reach their ends.
Inputs may be any that keep to these rules, and one draw needn't show every extreme that they name: `prompt_len`: the piece's tokens follow these cached positions. `step_lens`: each decoding token follows its sequence's cached positions.
All inputs are finite; a program needn't handle non-finite values.
Results may differ from the reference program's by a relative error of at most 0.015.
Values may be sent and summed in bfloat16 or wider, within the bound.
A program may use at most 128 MiB of HBM per device.

```python
import jax
import jax.numpy as jnp
from jax import lax

D = 4096
HEADS = 8
DH = 128
DV = 256
PIECE_DEV = 96
PCAP_DEV = 2048
DEC_DEV = 1
DCAP_DEV = 128
PIECE = 3072
PCAP = 65536
SEQS = 32
DEC_LEN = 4096
N_KV = 32
N_TP = 8


KEY_SCALE = 1.75


def base_keys(key, shape):
    return jnp.clip(jax.random.normal(key, shape, jnp.float32), -6.0, 6.0) * KEY_SCALE


def draw_prompt_keys(key, part):
    entries = base_keys(jax.random.fold_in(key, 3), (PCAP, HEADS, 2, DH))
    return entries.astype(jnp.bfloat16)


def draw_step_cache_keys(key, part):
    entries = base_keys(jax.random.fold_in(key, 7), (SEQS, DEC_LEN, HEADS, 2, DH))
    return entries.astype(jnp.bfloat16)


def touch_ends(array, own_key, smallest, top_value):
    longest = array.shape.index(max(array.shape))
    spots = []
    for shift in (0, 1):
        where = [jax.random.randint(jax.random.fold_in(own_key, axis), (), 0, length) for axis, length in enumerate(array.shape)]
        where[longest] = (where[longest] + shift) % array.shape[longest]
        spots.append(tuple(where))
    return array.at[spots[0]].set(smallest).at[spots[1]].set(top_value)


def block_levels(own_key, extent, pieces, low, high):
    gain = 1.0
    for dim, blocks in pieces:
        steps = jax.random.uniform(jax.random.fold_in(jax.random.fold_in(own_key, 6), dim), (blocks,), jnp.float32, low / len(pieces), high / len(pieces))
        gain = gain * jnp.repeat(jnp.exp(steps), extent[dim] // blocks).reshape((-1,) + (1,) * (len(extent) - 1 - dim))
    return gain


def noise(stream_key, dims, spread, limit, cuts=(), kind=jnp.bfloat16):
    values = spread * jax.random.normal(stream_key, dims, jnp.float32)
    if cuts:
        values = values * block_levels(stream_key, dims, cuts, -0.22, 0.18)
    return jnp.clip(values, -limit, limit).astype(kind)


def setup_inputs(seed: int = 0) -> dict:
    key_of = jax.random.split(jax.random.key(seed), 16)
    return {
        "piece_tokens": noise(key_of[0], (PIECE, D), 1.0, 6.0, ((0, 32),)),
        "step_tokens": noise(key_of[1], (SEQS, D), 1.0, 6.0, ((0, 32),)),
        "in_gain": jnp.clip(1.0 + 0.18 * jax.random.normal(key_of[2], (D,), jnp.float32), 0.1, 1.9),
        "w_query": noise(key_of[3], (D, HEADS, 2, DH), D ** -0.5, 0.09375, ((1, 8),)),
        "w_key": noise(key_of[4], (D, HEADS, 2, DH), (D // 3) ** -0.5, 0.15625, ((1, 8),)),
        "w_value": noise(key_of[5], (D, HEADS, DV), D ** -0.5, 0.09375, ((1, 8),)),
        "w_out": noise(key_of[6], (HEADS, DV, D), (HEADS * DV) ** -0.5, 0.125, ((0, 8),)),
        "mix_ratio": jnp.clip(0.3 + 0.5 * jax.random.uniform(key_of[7], (HEADS,), jnp.float32) ** block_levels(key_of[7], (HEADS,), ((0, 8),), -0.2, 0.2), 0.3, 0.8),
        "out_gain": jnp.clip(1.0 + 0.18 * jax.random.normal(key_of[8], (DV,), jnp.float32), 0.1, 1.9),
        "prompt_keys": draw_prompt_keys(jax.random.fold_in(key_of[15], 71), 0),
        "prompt_values": noise(key_of[10], (PCAP, HEADS, DV), 1.0, 6.0, ((0, 32), (1, 8))),
        "step_cache_keys": draw_step_cache_keys(jax.random.fold_in(key_of[15], 71), 0),
        "step_cache_values": noise(key_of[12], (SEQS, DEC_LEN, HEADS, DV), 1.0, 6.0, ((1, 32), (2, 8))),
        "prompt_len": jax.random.randint(key_of[13], (1,), PCAP - PCAP_DEV // 2, PCAP + 1).astype(jnp.int32),
        "step_lens": touch_ends(jax.random.randint(key_of[14], (SEQS,), DEC_LEN - DCAP_DEV // 2, DEC_LEN + 1), jax.random.fold_in(key_of[14], 1), DEC_LEN - DCAP_DEV // 2, DEC_LEN).astype(jnp.int32),
    }


EPS = 1e-06
OUT_SCALE = 0.8

def norm_rows(tokens, in_gain):
    floats = tokens.astype(jnp.float32)
    inv_rms = lax.rsqrt(lax.optimization_barrier(jnp.mean(floats * floats, axis=-1, keepdims=True)) + EPS)
    return (floats * inv_rms * in_gain.astype(jnp.float32)).astype(jnp.bfloat16)

def project(normed, weight):
    flat_weight = weight.reshape(weight.shape[0], -1)
    product = jnp.dot(normed, flat_weight, preferred_element_type=jnp.float32)
    rounded = lax.optimization_barrier(product.astype(jnp.bfloat16))
    return rounded.reshape((normed.shape[0],) + weight.shape[1:])

def head_partial(queries, key_rows, value_rows, visible):
    scores = jnp.einsum('qcd,kcd->cqk', queries.astype(jnp.float32), key_rows.astype(jnp.float32))
    scores = scores * queries.shape[-1] ** (-0.5)
    scores = jnp.where(visible[None], scores, -jnp.inf)
    maxima = lax.optimization_barrier(jnp.max(scores, axis=-1))
    weights = jnp.exp(scores - maxima[..., None])
    totals = lax.optimization_barrier(jnp.sum(weights, axis=-1))
    rounded = lax.optimization_barrier(weights.astype(jnp.bfloat16))
    summed = jnp.einsum('cqk,kv->qcv', rounded.astype(jnp.float32), value_rows.astype(jnp.float32))
    summed = lax.optimization_barrier(summed.astype(jnp.bfloat16))
    return (summed, jnp.transpose(maxima), jnp.transpose(totals))

def fold_group(running, summed, maxima, totals):
    row_best, norm_sum, value_sum = running
    new_best = jnp.maximum(row_best, maxima)
    old_scale = jnp.exp(row_best - new_best)
    new_scale = jnp.exp(maxima - new_best)
    return (new_best, norm_sum * old_scale + totals * new_scale, value_sum * old_scale[..., None] + summed.astype(jnp.float32) * new_scale[..., None])

def finish(norm_sum, value_sum, mix_ratio, out_gain):
    attended = value_sum / norm_sum[..., None]
    mixed = attended[:, :, 0] - mix_ratio[None, :, None] * attended[:, :, 1]
    inv_rms = lax.rsqrt(lax.optimization_barrier(jnp.mean(mixed * mixed, axis=-1, keepdims=True)) + EPS)
    return (mixed * inv_rms * out_gain[None, None, :] * OUT_SCALE).astype(jnp.bfloat16)

def empty_state(row_count):
    return (jnp.full((row_count, HEADS, 2), -jnp.inf, jnp.float32), jnp.zeros((row_count, HEADS, 2), jnp.float32), jnp.zeros((row_count, HEADS, 2, DV), jnp.float32))

def reference(piece_tokens, step_tokens, in_gain, w_query, w_key, w_value, w_out, mix_ratio, out_gain, prompt_keys, prompt_values, step_cache_keys, step_cache_values, prompt_len, step_lens):
    all_rows = jnp.concatenate([piece_tokens, step_tokens], axis=0)
    normed = norm_rows(all_rows, in_gain)
    queries = project(normed, w_query)
    key_rows = project(normed, w_key)
    value_rows = project(normed, w_value)
    piece_q = queries[:PIECE]
    step_q = queries[PIECE:]
    piece_k = key_rows[:PIECE]
    step_k = key_rows[PIECE:]
    piece_v = value_rows[:PIECE]
    step_v = value_rows[PIECE:]
    row_place = jnp.arange(PIECE, dtype=jnp.int32)
    seq_place = jnp.arange(SEQS, dtype=jnp.int32)

    def piece_group(running, group_id):
        cache_k = lax.dynamic_slice_in_dim(prompt_keys, group_id * PCAP_DEV, PCAP_DEV, 0)
        cache_v = lax.dynamic_slice_in_dim(prompt_values, group_id * PCAP_DEV, PCAP_DEV, 0)
        fresh_k = lax.dynamic_slice_in_dim(piece_k, group_id * PIECE_DEV, PIECE_DEV, 0)
        fresh_v = lax.dynamic_slice_in_dim(piece_v, group_id * PIECE_DEV, PIECE_DEV, 0)
        all_k = jnp.concatenate([cache_k, fresh_k], axis=0)
        all_v = jnp.concatenate([cache_v, fresh_v], axis=0)
        cache_place = group_id * PCAP_DEV + jnp.arange(PCAP_DEV, dtype=jnp.int32)
        fresh_place = group_id * PIECE_DEV + jnp.arange(PIECE_DEV, dtype=jnp.int32)
        visible = jnp.concatenate([jnp.broadcast_to((cache_place < prompt_len[0])[None, :], (PIECE, PCAP_DEV)), fresh_place[None, :] <= row_place[:, None]], axis=1)

        def one_head(operands):
            return head_partial(operands[0], operands[1], operands[2], visible)
        summed, maxima, totals = lax.map(one_head, (jnp.moveaxis(piece_q, 1, 0), jnp.moveaxis(all_k, 1, 0), jnp.moveaxis(all_v, 1, 0)))
        return (fold_group(running, jnp.moveaxis(summed, 0, 1), jnp.moveaxis(maxima, 0, 1), jnp.moveaxis(totals, 0, 1)), None)
    piece_state = lax.scan(piece_group, empty_state(PIECE), jnp.arange(N_KV, dtype=jnp.int32))[0]

    def step_group(running, group_id):
        cache_k = lax.dynamic_slice_in_dim(step_cache_keys, group_id * DCAP_DEV, DCAP_DEV, 1)
        cache_v = lax.dynamic_slice_in_dim(step_cache_values, group_id * DCAP_DEV, DCAP_DEV, 1)
        all_k = jnp.concatenate([cache_k, step_k[:, None]], axis=1)
        all_v = jnp.concatenate([cache_v, step_v[:, None]], axis=1)
        cache_place = group_id * DCAP_DEV + jnp.arange(DCAP_DEV, dtype=jnp.int32)
        visible = jnp.concatenate([cache_place[None, :] < step_lens[:, None], (seq_place // DEC_DEV == group_id)[:, None]], axis=1)
        scores = jnp.einsum('bhcd,bkhcd->bhck', step_q.astype(jnp.float32), all_k.astype(jnp.float32))
        scores = scores * DH ** (-0.5)
        scores = jnp.where(visible[:, None, None, :], scores, -jnp.inf)
        maxima = lax.optimization_barrier(jnp.max(scores, axis=-1))
        weights = jnp.exp(scores - maxima[..., None])
        totals = lax.optimization_barrier(jnp.sum(weights, axis=-1))
        rounded = lax.optimization_barrier(weights.astype(jnp.bfloat16))
        summed = jnp.einsum('bhck,bkhv->bhcv', rounded.astype(jnp.float32), all_v.astype(jnp.float32))
        summed = lax.optimization_barrier(summed.astype(jnp.bfloat16))
        return (fold_group(running, summed, maxima, totals), None)
    step_state = lax.scan(step_group, empty_state(SEQS), jnp.arange(N_KV, dtype=jnp.int32))[0]
    headout = jnp.concatenate([finish(piece_state[1], piece_state[2], mix_ratio, out_gain), finish(step_state[1], step_state[2], mix_ratio, out_gain)], axis=0)
    total_rows = PIECE + SEQS
    per_group = HEADS // N_TP
    grouped = jnp.moveaxis(headout.reshape(total_rows, N_TP, per_group * DV), 1, 0)
    weights = w_out.reshape(N_TP, per_group * DV, D)

    def group_term(operands):
        return jnp.dot(operands[0], operands[1], preferred_element_type=jnp.float32).astype(jnp.bfloat16)
    terms = lax.optimization_barrier(lax.map(group_term, (grouped, weights)))
    mixed = lax.optimization_barrier(jnp.sum(terms.astype(jnp.float32), axis=0)).astype(jnp.bfloat16)
    return (mixed[:PIECE], mixed[PIECE:], piece_k, piece_v, step_k, step_v)
```

```python
import functools
import math

import jax
import jax.numpy as jnp
from jax import lax
from jax.experimental import pallas as pl
from jax.experimental.pallas import tpu as pltpu
from jax.sharding import PartitionSpec as P

EPS = 1e-06
OUT_SCALE = 0.8
MESH = pl.DeviceIdType.MESH
HIDDEN = -1e30


def norm_rows(tokens, in_gain):
    floats = tokens.astype(jnp.float32)
    inv_rms = lax.rsqrt(jnp.mean(floats * floats, axis=-1, keepdims=True) + EPS)
    return (floats * inv_rms * in_gain).astype(jnp.bfloat16)


def project(normed, weight):
    order = tuple(range(1, weight.ndim - 1)) + (0, weight.ndim - 1)
    parts = jnp.transpose(weight, order)
    parts = parts.reshape((-1,) + parts.shape[-2:])
    product = jnp.einsum("nd,gdk->gnk", normed, parts, preferred_element_type=jnp.float32)
    return product.astype(jnp.bfloat16)


def meet(axis, count):
    me = lax.axis_index(axis)
    barrier = pltpu.get_barrier_semaphore()
    for step in range(1, count):
        pl.semaphore_signal(
            barrier, inc=1, device_id={axis: lax.rem(me + step, count)}, device_id_type=MESH
        )
    pl.semaphore_wait(barrier, count - 1)
    return me


def gather_kernel(axis, count, own, everyone, send_sem, recv_sem):
    me = meet(axis, count)
    copies = []
    for step in range(1, count):
        copy = pltpu.make_async_remote_copy(
            src_ref=own,
            dst_ref=everyone.at[me],
            send_sem=send_sem.at[step],
            recv_sem=recv_sem.at[step],
            device_id={axis: lax.rem(me + step, count)},
            device_id_type=MESH,
        )
        copy.start()
        copies.append(copy)
    everyone[me] = own[...]
    for copy in copies:
        copy.wait()


def gather_rows(own, axis, count, collective):
    return pl.pallas_call(
        functools.partial(gather_kernel, axis, count),
        out_shape=jax.ShapeDtypeStruct((count,) + own.shape, own.dtype),
        in_specs=[pl.BlockSpec(memory_space=pltpu.VMEM)],
        out_specs=pl.BlockSpec(memory_space=pltpu.VMEM),
        scratch_shapes=[
            pltpu.SemaphoreType.DMA((count,)),
            pltpu.SemaphoreType.DMA((count,)),
        ],
        compiler_params=pltpu.CompilerParams(collective_id=collective, has_side_effects=True),
        name="gather_rows",
    )(own)


def mix_maps(first, second, ratio, gain):
    mixed = first - ratio * second
    inv_rms = lax.rsqrt(jnp.mean(mixed * mixed, axis=-1, keepdims=True) + EPS)
    return (mixed * inv_rms * gain * OUT_SCALE).astype(jnp.bfloat16)


def blend(values, tops, totals):
    count = len(values)
    best = functools.reduce(jnp.maximum, tops)
    scales = [jnp.exp(top - best) for top in tops]
    norm = functools.reduce(jnp.add, [scales[g] * totals[g] for g in range(count)])
    total = functools.reduce(jnp.add, [values[g] * scales[g] for g in range(count)])
    return total / norm


SIDE_Y = 4
TILE = 128


def spread(stats, first, groups, width):
    cols = [jnp.broadcast_to(stats[:, i : i + 1], (8, width)) for i in range(first, first + groups)]
    return jnp.concatenate(cols, axis=0)


def pack_columns(columns):
    lane = lax.broadcasted_iota(jnp.int32, (8, TILE), 1)
    out = jnp.zeros((8, TILE), jnp.float32)
    for place, column in columns:
        out = jnp.where(lane == place, column, out)
    return out


def ring_kernel(
    kv_count, fold, ratio, gain, q_own, kt, values, bias, step, out,
    q_all, scores, weights, sent_v, sent_s, got_v, got_s, far_v, far_s, all_t,
    qz_send, qz_recv, qy_send, qy_recv, r_send, r_recv, f_send, f_recv, t_send, t_recv,
):
    ny = SIDE_Y
    nz = kv_count // ny
    rows, dims = q_own.shape[1:]
    wide = values.shape[1]
    cached = bias.shape[1]
    total_keys = values.shape[0]
    half = 2 * rows
    blocks = rows // 8
    me = lax.axis_index("kv")
    z = me // ny
    y = lax.rem(me, ny)
    other_z = [lax.rem(z + 1, nz) * ny + y, lax.rem(z + nz - 1, nz) * ny + y]

    def to(src, dst, send, recv, device):
        return pltpu.make_async_remote_copy(
            src_ref=src, dst_ref=dst, send_sem=send, recv_sem=recv,
            device_id={"kv": device}, device_id_type=MESH,
        )

    def along_z(m, slot, source):
        return to(source, q_all.at[m, slot, y], qz_send.at[m, slot], qz_recv.at[m, slot], other_z[m])

    def along_y(m, slot, turn, source):
        return to(
            source, q_all.at[m, slot, y], qy_send.at[m, slot, turn], qy_recv.at[m, slot, y],
            z * ny + lax.rem(y + turn, ny),
        )

    def from_y(m, slot, turn):
        there = lax.rem(y + turn, ny)
        return to(
            q_all.at[m, slot, there], q_all.at[m, slot, there],
            qy_send.at[m, slot, turn], qy_recv.at[m, slot, there], z * ny + there,
        )

    def ring(m, slot, h):
        at = pl.ds(h * half, half)
        return (
            to(sent_s.at[m, slot, h], got_s.at[m, slot + 1, h],
               r_send.at[m, slot, h, 0], r_recv.at[m, slot, h, 0], other_z[m]),
            to(sent_v.at[m, slot, at], got_v.at[m, slot + 1, at],
               r_send.at[m, slot, h, 1], r_recv.at[m, slot, h, 1], other_z[m]),
        )

    def final(m, there):
        at = pl.ds(pl.multiple_of(there * rows, 32), rows)
        return (
            to(sent_s.at[m, nz - 1, there // 2], far_s.at[m, y],
               f_send.at[m, there, 0], f_recv.at[m, y, 0], z * ny + there),
            to(sent_v.at[m, nz - 1, at], far_v.at[m, y],
               f_send.at[m, there, 1], f_recv.at[m, y, 1], z * ny + there),
        )

    def final_from(m, there):
        return (
            to(far_s.at[m, there], far_s.at[m, there],
               f_send.at[m, there, 0], f_recv.at[m, there, 0], z * ny + there),
            to(far_v.at[m, there], far_v.at[m, there],
               f_send.at[m, there, 1], f_recv.at[m, there, 1], z * ny + there),
        )

    meet("kv", kv_count)
    for m in range(2):
        along_z(m, 0, q_own.at[m]).start()
    for m in range(2):
        for turn in range(1, ny):
            along_y(m, nz - 1, turn, q_own.at[m]).start()
    step_copies = []
    for turn in range(1, kv_count):
        there = lax.rem(me + turn, kv_count)
        copy = to(step.at[there], all_t.at[me], t_send.at[turn], t_recv.at[turn], there)
        copy.start()
        step_copies.append(copy)
    all_t[me] = step[me]
    for m in range(2):
        q_all[m, nz - 1, y] = q_own[m]
        got_v[m, 0] = jnp.zeros(got_v.shape[2:], jnp.bfloat16)
        lane = lax.broadcasted_iota(jnp.int32, (8, TILE), 1)
        tops = lax.rem(lane, 2 * blocks) < blocks
        for h in range(2):
            got_s[m, 0, h] = jnp.where(tops, HIDDEN, 0.0)

    def pass_on(slot):
        for m in range(2):
            along_z(m, slot, q_own.at[m]).wait_recv()

            @pl.when(slot < nz - 2)
            def _():
                along_z(m, slot + 1, q_all.at[m, slot, y]).start()

            for turn in range(1, ny):
                along_y(m, slot, turn, q_all.at[m, slot, y]).start()

    pass_on(0)

    def score(m, h, slot, off):
        q = q_all[m, slot, 2 * h : 2 * h + 2].reshape(half, dims)
        buf = (2 * m + h) % 2
        best = None
        for c in range(0, cached, 256):
            s = jnp.dot(q, kt[m, :, c : c + 256], preferred_element_type=jnp.float32)
            s = s + bias[:, c : c + 256]
            scores[buf, :, c : c + 256] = s
            for j in range(0, 256, TILE):
                p = s[:, j : j + TILE]
                best = p if best is None else jnp.maximum(best, p)
        tail = jnp.dot(q, kt[m, :, cached:], preferred_element_type=jnp.float32)
        lane = lax.broadcasted_iota(jnp.int32, tail.shape, 1)
        row = lax.broadcasted_iota(jnp.int32, tail.shape, 0)
        gap = jnp.where(lane < rows, lane - row, 1 << 20)
        tail = jnp.where(gap <= off, tail, HIDDEN)
        scores[buf, :, cached:] = tail
        best = jnp.maximum(best, tail)
        return jnp.max(best, axis=1, keepdims=True)

    def weigh(m, h, top):
        buf = (2 * m + h) % 2
        part = None
        for c in range(0, total_keys, TILE):
            w = jnp.exp2((scores[buf, :, c : c + TILE] - top) * fold)
            weights[buf, :, c : c + TILE] = w.astype(jnp.bfloat16)
            part = w if part is None else part + w
        total = jnp.sum(part, axis=1, keepdims=True)
        return jnp.dot(weights[buf], values[...], preferred_element_type=jnp.float32), total

    def join(m, h, slot, top, total, summed):
        at = pl.ds(h * half, half)
        old = got_s[m, slot, h]
        old_top = jnp.concatenate([spread(old, 2 * blocks * j, blocks, TILE) for j in range(2)], axis=0)
        old_total = jnp.concatenate(
            [spread(old, 2 * blocks * j + blocks, blocks, TILE) for j in range(2)], axis=0
        )
        best = jnp.maximum(old_top, top)
        old_scale = jnp.exp2((old_top - best) * fold)
        new_scale = jnp.exp2((top - best) * fold)
        norm = old_total * old_scale + total * new_scale
        for c in range(0, wide, TILE):
            mixed = got_v[m, slot, at, c : c + TILE].astype(jnp.float32) * old_scale
            mixed = mixed + summed[:, c : c + TILE] * new_scale
            sent_v[m, slot, at, c : c + TILE] = mixed.astype(jnp.bfloat16)
        columns = []
        for j in range(2):
            for i in range(blocks):
                line = slice(j * rows + i * 8, j * rows + i * 8 + 8)
                columns.append((2 * blocks * j + i, best[line]))
                columns.append((2 * blocks * j + blocks + i, norm[line]))
        sent_s[m, slot, h] = pack_columns(columns)

    units = [(m, h) for m in range(2) for h in range(2)]

    def turn_step(slot, carry):
        @pl.when(slot < nz - 2)
        def _():
            pass_on(slot + 1)

        for m in range(2):
            for turn in range(1, ny):
                from_y(m, slot, turn).wait_recv()
        homes = [lax.rem(z + nz - 1 - slot, nz), lax.rem(z + 1 + slot, nz)]
        offs = [[(homes[m] * ny + 2 * h - me) * rows for h in range(2)] for m in range(2)]
        tops = [None] * len(units)
        tops[0] = score(0, 0, slot, offs[0][0])
        for u, (m, h) in enumerate(units):
            if u + 1 < len(units):
                m2, h2 = units[u + 1]
                tops[u + 1] = score(m2, h2, slot, offs[m2][h2])
            summed, total = weigh(m, h, tops[u])

            @pl.when(slot > 0)
            def _():
                for copy in ring(m, slot - 1, h):
                    copy.wait_recv()

            join(m, h, slot, tops[u], total, summed)

            @pl.when(slot < nz - 1)
            def _():
                for copy in ring(m, slot, h):
                    copy.start()

            @pl.when(slot == nz - 1)
            def _():
                for there in range(2 * h, 2 * h + 2):
                    @pl.when(y != there)
                    def _():
                        for copy in final(m, there):
                            copy.start()
        return carry

    lax.fori_loop(0, nz, turn_step, 0)

    for copy in step_copies:
        copy.wait()
    low = out.shape[0] - rows
    maps_out = []
    for m in range(2):
        maps_out.append(
            blend(
                [all_t[g, m : m + 1, :wide] for g in range(kv_count)],
                [all_t[g, m : m + 1, wide : wide + 1] for g in range(kv_count)],
                [all_t[g, m : m + 1, wide + 1 : wide + 2] for g in range(kv_count)],
            )
        )
    line = mix_maps(maps_out[0], maps_out[1], ratio[0, 0], gain[...]).astype(jnp.float32)
    place = lax.broadcasted_iota(jnp.int32, (low, wide), 0)
    out[rows:, :] = jnp.where(place == 0, line, 0.0).astype(jnp.bfloat16)

    for m in range(2):
        for turn in range(1, ny):
            for copy in final_from(m, lax.rem(y + turn, ny)):
                copy.wait_recv()
    odd = lax.rem(y, 2) == 1

    def own_half(stats):
        return jnp.where(odd, pltpu.roll(stats, TILE - 2 * blocks, 1), stats)

    stats = [
        [own_half(sent_s[m, nz - 1, y // 2])]
        + [own_half(far_s[m, lax.rem(y + turn, ny)]) for turn in range(1, ny)]
        for m in range(2)
    ]
    tall = 32
    for j in range(rows // tall):
        maps_out = []
        for m in range(2):
            at = pl.ds(pl.multiple_of(y * rows + j * tall, tall), tall)
            vals = [sent_v[m, nz - 1, at, :]]
            vals += [far_v[m, lax.rem(y + turn, ny), j * tall : (j + 1) * tall, :] for turn in range(1, ny)]
            tops = [spread(s, j * tall // 8, tall // 8, wide) for s in stats[m]]
            totals = [spread(s, blocks + j * tall // 8, tall // 8, wide) for s in stats[m]]
            best = functools.reduce(jnp.maximum, tops)
            scales = [jnp.exp2((t - best) * fold) for t in tops]
            norm = functools.reduce(jnp.add, [a * b for a, b in zip(scales, totals)])
            total = functools.reduce(jnp.add, [a * b.astype(jnp.float32) for a, b in zip(scales, vals)])
            maps_out.append(total / norm)
        out[j * tall : (j + 1) * tall, :] = mix_maps(maps_out[0], maps_out[1], ratio[0, 0], gain[...])

    for m in range(2):
        for there in range(ny):
            @pl.when(y != there)
            def _():
                for copy in final(m, there):
                    copy.wait_send()
        for turn in range(1, ny):
            along_y(m, nz - 1, turn, q_own.at[m]).wait_send()

    def drain(slot, carry):
        for m in range(2):
            along_z(m, slot, q_own.at[m]).wait_send()
            for turn in range(1, ny):
                along_y(m, slot, turn, q_own.at[m]).wait_send()
            for h in range(2):
                for copy in ring(m, slot, h):
                    copy.wait_send()
        return carry

    lax.fori_loop(0, nz - 1, drain, 0)


def ring_attend(q_own, kt, values, bias, step, ratio, gain, kv_count, padded, collective):
    rows, dims = q_own.shape[1:]
    wide = values.shape[1]
    keys = values.shape[0]
    ny = SIDE_Y
    nz = kv_count // ny
    vmem = pl.BlockSpec(memory_space=pltpu.VMEM)
    dma = pltpu.SemaphoreType.DMA
    fold = dims ** (-0.5) * math.log2(math.e)
    return pl.pallas_call(
        functools.partial(ring_kernel, kv_count, fold),
        out_shape=jax.ShapeDtypeStruct((padded, wide), jnp.bfloat16),
        in_specs=[pl.BlockSpec(memory_space=pltpu.SMEM)] + [vmem] * 6,
        out_specs=vmem,
        scratch_shapes=[
            pltpu.VMEM((2, nz, ny, rows, dims), jnp.bfloat16),
            pltpu.VMEM((2, 2 * rows, keys), jnp.float32),
            pltpu.VMEM((2, 2 * rows, keys), jnp.bfloat16),
            pltpu.VMEM((2, nz, ny * rows, wide), jnp.bfloat16),
            pltpu.VMEM((2, nz, 2, 8, TILE), jnp.float32),
            pltpu.VMEM((2, nz, ny * rows, wide), jnp.bfloat16),
            pltpu.VMEM((2, nz, 2, 8, TILE), jnp.float32),
            pltpu.VMEM((2, ny, rows, wide), jnp.bfloat16),
            pltpu.VMEM((2, ny, 8, TILE), jnp.float32),
            pltpu.VMEM(step.shape, step.dtype),
            dma((2, nz)), dma((2, nz)),
            dma((2, nz, ny)), dma((2, nz, ny)),
            dma((2, nz, 2, 2)), dma((2, nz, 2, 2)),
            dma((2, ny, 2)), dma((2, ny, 2)),
            dma((kv_count,)), dma((kv_count,)),
        ],
        compiler_params=pltpu.CompilerParams(
            collective_id=collective, has_side_effects=True, vmem_limit_bytes=56 * 1024 * 1024
        ),
        name="ring_attend",
    )(ratio, gain, q_own, kt, values, bias, step)


def project_out_kernel(axis, count, heads, weight, out, terms, pair, half, far, d_send, d_recv, x_send, x_recv):
    me = lax.axis_index(axis)
    chips = count // 2
    chip, core = me // 2, lax.rem(me, 2)
    meet(axis, count)
    wide = out.shape[1]
    for target in range(count):
        terms[target] = jnp.dot(
            heads[...], weight[:, target * wide : target * wide + wide], preferred_element_type=jnp.float32
        ).astype(jnp.bfloat16)
    near = []
    for turn in range(1, chips + 1):
        there = lax.rem(chip + turn, chips)
        copy = pltpu.make_async_remote_copy(
            src_ref=terms.at[there * 2 + 1 - core],
            dst_ref=pair.at[there],
            send_sem=d_send.at[turn],
            recv_sem=d_recv.at[turn],
            device_id={axis: chip * 2 + 1 - core},
            device_id_type=MESH,
        )
        copy.start()
        near.append(copy)
    away = []
    for turn in range(1, chips + 1):
        near[turn - 1].wait()
        there = lax.rem(chip + turn, chips)
        both = terms[there * 2 + core].astype(jnp.float32) + pair[there].astype(jnp.float32)
        if turn == chips:
            total = both
            for copy in away:
                copy.wait()
            for slot in range(1, chips):
                total = total + far[slot].astype(jnp.float32)
            out[...] = total.astype(jnp.bfloat16)
        else:
            half[turn] = both.astype(jnp.bfloat16)
            copy = pltpu.make_async_remote_copy(
                src_ref=half.at[turn],
                dst_ref=far.at[turn],
                send_sem=x_send.at[turn],
                recv_sem=x_recv.at[turn],
                device_id={axis: there * 2 + core},
                device_id_type=MESH,
            )
            copy.start()
            away.append(copy)


def project_out(heads, weight, axis, count, collective):
    wide = weight.shape[1] // count
    rows = heads.shape[0]
    chips = count // 2
    vmem = pl.BlockSpec(memory_space=pltpu.VMEM)
    return pl.pallas_call(
        functools.partial(project_out_kernel, axis, count),
        out_shape=jax.ShapeDtypeStruct((rows, wide), jnp.bfloat16),
        in_specs=[vmem, vmem],
        out_specs=vmem,
        scratch_shapes=[
            pltpu.VMEM((count, rows, wide), jnp.bfloat16),
            pltpu.VMEM((chips, rows, wide), jnp.bfloat16),
            pltpu.VMEM((chips, rows, wide), jnp.bfloat16),
            pltpu.VMEM((chips, rows, wide), jnp.bfloat16),
            pltpu.SemaphoreType.DMA((chips + 1,)),
            pltpu.SemaphoreType.DMA((chips + 1,)),
            pltpu.SemaphoreType.DMA((chips + 1,)),
            pltpu.SemaphoreType.DMA((chips + 1,)),
        ],
        compiler_params=pltpu.CompilerParams(
            collective_id=collective, has_side_effects=True, vmem_limit_bytes=56 * 1024 * 1024
        ),
        name="project_out",
    )(heads, weight)


def on_device(
    kv_count,
    tp_count,
    piece_tokens,
    step_tokens,
    in_gain,
    w_query,
    w_key,
    w_value,
    w_out,
    mix_ratio,
    out_gain,
    prompt_keys,
    prompt_values,
    step_cache_keys,
    step_cache_values,
    prompt_len,
    step_lens,
):
    kv_place = lax.axis_index("kv")
    piece_dev = piece_tokens.shape[0]
    step_dev = step_tokens.shape[0]
    cache_dev = prompt_keys.shape[0]
    seq_count = step_cache_keys.shape[0]
    seq_cache = step_cache_keys.shape[1]
    heads, maps, dims = w_query.shape[1:]
    wide = w_value.shape[-1]
    parts = heads * maps
    padded = -(-(piece_dev + step_dev) // 16) * 16
    spare = jnp.zeros((padded - piece_dev - step_dev, piece_tokens.shape[1]), jnp.bfloat16)
    all_rows = jnp.concatenate([piece_tokens, step_tokens, spare], axis=0)
    normed = norm_rows(all_rows, in_gain)
    queries = project(normed, w_query)
    key_rows = project(normed, w_key)
    value_rows = project(normed, w_value)
    step_flat = queries[:, piece_dev].astype(jnp.float32)
    q_all = gather_rows(step_flat, "kv", kv_count, 0)
    end = piece_dev + step_dev

    def rows_of(flat, start, stop, extra):
        return jnp.transpose(flat[:, start:stop], (1, 0, 2)).reshape((stop - start,) + extra)

    piece_k = rows_of(key_rows, 0, piece_dev, (heads, maps, dims))
    step_k = rows_of(key_rows, piece_dev, end, (heads, maps, dims))
    piece_v = rows_of(value_rows, 0, piece_dev, (heads, wide))
    step_v = rows_of(value_rows, piece_dev, end, (heads, wide))
    spare_keys = -(-piece_dev // TILE) * TILE - piece_dev
    keys = jnp.transpose(prompt_keys, (1, 2, 3, 0)).reshape(parts, dims, cache_dev)
    fresh_k = jnp.transpose(key_rows[:, :piece_dev], (0, 2, 1))
    kt = jnp.concatenate([keys, fresh_k, jnp.zeros((parts, dims, spare_keys), jnp.bfloat16)], axis=2)
    all_v = jnp.concatenate(
        [prompt_values[:, 0], value_rows[0, :piece_dev], jnp.zeros((spare_keys, wide), jnp.bfloat16)], axis=0
    )
    cache_ok = kv_place * cache_dev + jnp.arange(cache_dev, dtype=jnp.int32) < prompt_len[0]
    bias = jnp.where(cache_ok, 0.0, HIDDEN)[None, :]
    step_q = q_all.astype(jnp.bfloat16).reshape(seq_count, heads, maps, dims)
    own_seq = jnp.arange(seq_count, dtype=jnp.int32) // step_dev == kv_place
    own_k = lax.dynamic_update_slice_in_dim(
        jnp.zeros((seq_count,) + step_k.shape[1:], jnp.bfloat16), step_k, kv_place * step_dev, 0
    )
    own_v = lax.dynamic_update_slice_in_dim(
        jnp.zeros((seq_count,) + step_v.shape[1:], jnp.bfloat16), step_v, kv_place * step_dev, 0
    )
    head_scale = step_q.shape[-1] ** (-0.5)
    cache_scores = (
        jnp.einsum("bhcd,bkhcd->bhck", step_q, step_cache_keys, preferred_element_type=jnp.float32)
        * head_scale
    )
    fresh_scores = (
        jnp.einsum("bhcd,bhcd->bhc", step_q, own_k, preferred_element_type=jnp.float32) * head_scale
    )
    cache_place = kv_place * seq_cache + jnp.arange(seq_cache, dtype=jnp.int32)
    cache_visible = cache_place[None, :] < step_lens[:, None]
    cache_scores = jnp.where(cache_visible[:, None, None, :], cache_scores, -jnp.inf)
    fresh_scores = jnp.where(own_seq[:, None, None], fresh_scores, -jnp.inf)
    step_max = jnp.maximum(jnp.max(cache_scores, axis=-1), fresh_scores)
    cache_weights = jnp.exp(cache_scores - step_max[..., None])
    fresh_weights = jnp.exp(fresh_scores - step_max)
    step_tot = jnp.sum(cache_weights, axis=-1) + fresh_weights
    fresh_rounded = lax.optimization_barrier(fresh_weights.astype(jnp.bfloat16))
    step_acc = jnp.einsum(
        "bhck,bkhv->bhcv",
        cache_weights.astype(jnp.bfloat16),
        step_cache_values,
        preferred_element_type=jnp.float32,
    )
    step_acc = (
        step_acc
        + fresh_rounded.astype(jnp.float32)[..., None] * own_v.astype(jnp.float32)[:, :, None, :]
    )
    step_sum = lax.optimization_barrier(step_acc.astype(jnp.bfloat16))
    message = jnp.concatenate(
        [
            step_sum.astype(jnp.float32),
            step_max[..., None],
            step_tot[..., None],
            jnp.zeros(step_tot.shape + (126,), jnp.float32),
        ],
        axis=-1,
    ).reshape(kv_count, step_dev * parts, wide + 128)
    flat_heads = ring_attend(
        queries[:, :piece_dev], kt, all_v, bias, message, mix_ratio[None, :], out_gain[None, :], kv_count, padded, 1
    )
    mixed = project_out(flat_heads, w_out.reshape(-1, w_out.shape[-1]), "tp", tp_count, 2)
    return (mixed[:piece_dev], mixed[piece_dev:end], piece_k, piece_v, step_k, step_v)


def solution(mesh):
    in_specs = (
        P("kv", None),
        P("kv", None),
        P(),
        P(None, "tp", None, None),
        P(None, "tp", None, None),
        P(None, "tp", None),
        P("tp", None, None),
        P("tp"),
        P(),
        P("kv", "tp", None, None),
        P("kv", "tp", None),
        P(None, "kv", "tp", None, None),
        P(None, "kv", "tp", None),
        P(),
        P(),
    )
    out_specs = (
        P("kv", "tp"),
        P("kv", "tp"),
        P("kv", "tp", None, None),
        P("kv", "tp", None),
        P("kv", "tp", None, None),
        P("kv", "tp", None),
    )
    return jax.shard_map(
        functools.partial(on_device, mesh.shape["kv"], mesh.shape["tp"]),
        mesh=mesh, in_specs=in_specs, out_specs=out_specs, check_vma=False
    )
```

```python
import functools
import math

import jax
import jax.numpy as jnp
from jax import lax
from jax.experimental import pallas as pl
from jax.experimental.pallas import tpu as pltpu
from jax.sharding import PartitionSpec as P

EPS = 1e-06
OUT_SCALE = 0.8
MESH = pl.DeviceIdType.MESH
HIDDEN = -1e30


def norm_rows(tokens, in_gain):
    floats = tokens.astype(jnp.float32)
    inv_rms = lax.rsqrt(jnp.mean(floats * floats, axis=-1, keepdims=True) + EPS)
    return (floats * inv_rms * in_gain).astype(jnp.bfloat16)


def project(normed, weight):
    order = tuple(range(1, weight.ndim - 1)) + (0, weight.ndim - 1)
    parts = jnp.transpose(weight, order)
    parts = parts.reshape((-1,) + parts.shape[-2:])
    product = jnp.einsum("nd,gdk->gnk", normed, parts, preferred_element_type=jnp.float32)
    return product.astype(jnp.bfloat16)


def meet(axis, count):
    me = lax.axis_index(axis)
    barrier = pltpu.get_barrier_semaphore()
    for step in range(1, count):
        pl.semaphore_signal(
            barrier, inc=1, device_id={axis: lax.rem(me + step, count)}, device_id_type=MESH
        )
    pl.semaphore_wait(barrier, count - 1)
    return me


def mix_maps(first, second, ratio, gain):
    mixed = first - ratio * second
    inv_rms = lax.rsqrt(jnp.mean(mixed * mixed, axis=-1, keepdims=True) + EPS)
    return (mixed * inv_rms * gain * OUT_SCALE).astype(jnp.bfloat16)


SIDE_Y = 4
TILE = 128
EXTRA = 16


def spread(stats, first, groups, width):
    cols = [jnp.broadcast_to(stats[:, i : i + 1], (8, width)) for i in range(first, first + groups)]
    return jnp.concatenate(cols, axis=0)


def pack_columns(columns):
    lane = lax.broadcasted_iota(jnp.int32, (8, TILE), 1)
    out = jnp.zeros((8, TILE), jnp.float32)
    for place, column in columns:
        out = jnp.where(lane == place, column, out)
    return out


def ring_kernel(
    kv_count, fold, ratio, prompt_len, step_lens, gain, queries, new_keys, new_values,
    prompt_keys, prompt_values, cache_keys, cache_values, out,
    q_own, q_all, pairs, kt, values, bias, halves, step_k, step_v, scores, weights,
    sent_v, sent_s, got_v, got_s, far_v, far_s, far_d,
    load_sem, qz_send, qz_recv, qy_send, qy_recv, r_send, r_recv, f_send, f_recv,
):
    ny = SIDE_Y
    nz = kv_count // ny
    tall, dims = queries.shape[1:]
    rows = tall - EXTRA
    wide = values.shape[1]
    cached = bias.shape[1]
    total_keys = values.shape[0]
    slots = step_v.shape[0] // kv_count
    half = 2 * rows
    blocks = rows // 8
    deep = 2 * half
    me = lax.axis_index("kv")
    z = me // ny
    y = lax.rem(me, ny)
    other_z = [lax.rem(z + 1, nz) * ny + y, lax.rem(z + nz - 1, nz) * ny + y]

    loads = [
        pltpu.make_async_copy(prompt_keys, pairs, load_sem.at[0]),
        pltpu.make_async_copy(prompt_values, values.at[pl.ds(0, cached)], load_sem.at[1]),
        pltpu.make_async_copy(cache_keys, step_k, load_sem.at[2]),
        pltpu.make_async_copy(cache_values, step_v, load_sem.at[3]),
    ]
    for copy in loads:
        copy.start()

    barrier = pltpu.get_barrier_semaphore()
    for turn in range(1, nz):
        there = lax.rem(z + turn, nz) * ny + y
        pl.semaphore_signal(barrier, inc=1, device_id={"kv": there}, device_id_type=MESH)
    for turn in range(1, ny):
        there = z * ny + lax.rem(y + turn, ny)
        pl.semaphore_signal(barrier, inc=1, device_id={"kv": there}, device_id_type=MESH)

    extra_row = lax.broadcasted_iota(jnp.int32, (EXTRA, dims), 0)
    for m in range(2):
        q_own[m, :rows] = queries[m, :rows]
        line = queries[m, rows:].astype(jnp.float32)[:1]
        q_own[m, rows:] = jnp.where(extra_row == y, line, 0.0).astype(jnp.bfloat16)
        q_all[m, nz - 1, y] = q_own[m]
        got_v[m, 0] = jnp.zeros(got_v.shape[2:], jnp.bfloat16)
        lane = lax.broadcasted_iota(jnp.int32, (8, TILE), 1)
        spot = jnp.where(lane < 4 * blocks, lax.rem(lane, 2 * blocks), lane - 4 * blocks + blocks - 2)
        for h in range(2):
            got_s[m, 0, h] = jnp.where(spot < blocks, HIDDEN, 0.0)

    pl.semaphore_wait(barrier, nz + ny - 2)

    def to(src, dst, send, recv, device):
        return pltpu.make_async_remote_copy(
            src_ref=src, dst_ref=dst, send_sem=send, recv_sem=recv,
            device_id={"kv": device}, device_id_type=MESH,
        )

    def along_z(m, slot):
        there = lax.rem(z + (1 + slot if m == 0 else nz - 1 - slot), nz) * ny + y
        return to(q_own.at[m], q_all.at[m, slot, y], qz_send.at[m, slot], qz_recv.at[m, slot], there)

    def along_y(m, slot, turn, source):
        return to(
            source, q_all.at[m, slot, y], qy_send.at[m, slot, turn], qy_recv.at[m, slot, y],
            z * ny + lax.rem(y + turn, ny),
        )

    def from_y(m, slot, turn):
        there = lax.rem(y + turn, ny)
        return to(
            q_all.at[m, slot, there], q_all.at[m, slot, there],
            qy_send.at[m, slot, turn], qy_recv.at[m, slot, there], z * ny + there,
        )

    def ring(m, slot, h):
        at = pl.ds(h * half, half + h * EXTRA)
        return (
            to(sent_s.at[m, slot, h], got_s.at[m, slot + 1, h],
               r_send.at[m, slot, h, 0], r_recv.at[m, slot, h, 0], other_z[m]),
            to(sent_v.at[m, slot, at], got_v.at[m, slot + 1, at],
               r_send.at[m, slot, h, 1], r_recv.at[m, slot, h, 1], other_z[m]),
        )

    def final(m, there, i):
        at = pl.ds(pl.multiple_of(there * rows, 32), rows)
        low = pl.ds(deep, EXTRA)
        peer = z * ny + there
        src = (sent_v.at[m, nz - 1, at], sent_s.at[m, nz - 1], sent_v.at[m, nz - 1, low])[i]
        dst = (far_v, far_s, far_d)[i].at[m, y]
        return to(src, dst, f_send.at[m, there, i], f_recv.at[m, y, i], peer)

    def final_from(m, there):
        peer = z * ny + there
        return tuple(
            to(ref.at[m, there], ref.at[m, there], f_send.at[m, there, i], f_recv.at[m, there, i], peer)
            for i, ref in enumerate((far_v, far_s, far_d))
        )

    for m in range(2):
        along_z(m, 0).start()
    for m in range(2):
        along_z(m, 1).start()
    for slot in range(2, nz - 1):
        for m in range(2):
            along_z(m, slot).start()
    for m in range(2):
        for turn in range(1, ny):
            along_y(m, nz - 1, turn, q_own.at[m]).start()

    def fan_out(slot):
        for m in range(2):
            along_z(m, slot).wait_recv()
            for turn in range(1, ny):
                along_y(m, slot, turn, q_all.at[m, slot, y]).start()

    fan_out(0)

    key_lane = lax.broadcasted_iota(jnp.int32, (1, cached), 1)
    bias[...] = jnp.where(me * cached + key_lane < prompt_len[0], 0.0, HIDDEN)
    values[cached : cached + rows] = new_values[:rows]
    values[cached + rows :] = jnp.zeros((total_keys - cached - rows, wide), jnp.bfloat16)
    for m in range(2):
        fresh = jnp.concatenate(
            [new_keys[m, :rows].astype(jnp.float32), jnp.zeros((TILE - rows, dims), jnp.float32)], axis=0
        )
        kt[m, :, cached:] = jnp.transpose(fresh).astype(jnp.bfloat16)
    up = lax.broadcasted_iota(jnp.int32, (2 * TILE, 2 * TILE), 0)
    across = lax.broadcasted_iota(jnp.int32, (2 * TILE, 2 * TILE), 1)
    sort = jnp.where(across < TILE, 2 * across, 2 * across - 2 * TILE + 1) == up
    sort = sort.astype(jnp.float32).astype(jnp.bfloat16)
    up = lax.broadcasted_iota(jnp.int32, (2 * TILE, TILE), 0)
    across = lax.broadcasted_iota(jnp.int32, (2 * TILE, TILE), 1)
    halves[...] = (up // 2 == across).astype(jnp.float32).astype(jnp.bfloat16)
    loads[0].wait()

    def split(i, carry):
        block = pairs[pl.ds(pl.multiple_of(i * 2 * TILE, 2 * TILE), 2 * TILE), :]
        turned = lax.dot_general(
            block, sort, (((0,), (0,)), ((), ())), preferred_element_type=jnp.float32
        ).astype(jnp.bfloat16)
        at = pl.ds(pl.multiple_of(i * TILE, TILE), TILE)
        kt[0, :, at] = turned[:, :TILE]
        kt[1, :, at] = turned[:, TILE:]
        return carry

    lax.fori_loop(0, cached // TILE, split, 0)
    for copy in loads[1:]:
        copy.wait()

    def score(m, h, slot, off):
        q = q_all[m, slot, 2 * h : 2 * h + 2, :rows].reshape(half, dims)
        buf = (2 * m + h) % 2
        best = None
        for c in range(0, cached, 256):
            s = jnp.dot(q, kt[m, :, c : c + 256], preferred_element_type=jnp.float32)
            s = s + bias[:, c : c + 256]
            scores[buf, :, c : c + 256] = s
            for j in range(0, 256, TILE):
                p = s[:, j : j + TILE]
                best = p if best is None else jnp.maximum(best, p)
        tail = jnp.dot(q, kt[m, :, cached:], preferred_element_type=jnp.float32)
        lane = lax.broadcasted_iota(jnp.int32, tail.shape, 1)
        row = lax.broadcasted_iota(jnp.int32, tail.shape, 0)
        gap = jnp.where(lane < rows, lane - row, 1 << 20)
        tail = jnp.where(gap <= off, tail, HIDDEN)
        scores[buf, :, cached:] = tail
        best = jnp.maximum(best, tail)
        return jnp.max(best, axis=1, keepdims=True)

    def weigh(m, h, top):
        buf = (2 * m + h) % 2
        part = None
        for c in range(0, total_keys, TILE):
            w = jnp.exp2((scores[buf, :, c : c + TILE] - top) * fold)
            weights[buf, :, c : c + TILE] = w.astype(jnp.bfloat16)
            part = w if part is None else part + w
        total = jnp.sum(part, axis=1, keepdims=True)
        return jnp.dot(weights[buf], values[...], preferred_element_type=jnp.float32), total

    def decode(m, slot, home):
        q = q_all[m, slot, 0, rows:].astype(jnp.float32)
        for there in range(1, ny):
            q = q + q_all[m, slot, there, rows:].astype(jnp.float32)
        qb = q.astype(jnp.bfloat16)
        row = lax.broadcasted_iota(jnp.int32, (EXTRA, 2 * slots), 0)
        lane = lax.broadcasted_iota(jnp.int32, (EXTRA, 2 * slots), 1)
        s = jnp.zeros((EXTRA, 2 * slots), jnp.float32)
        lens = jnp.zeros((EXTRA, 2 * slots), jnp.int32)
        for there in range(ny):
            seq = home * ny + there
            at = pl.ds(pl.multiple_of(seq * 2 * slots, 2 * slots), 2 * slots)
            one = lax.dot_general(
                qb, step_k[at, :], (((1,), (1,)), ((), ())), preferred_element_type=jnp.float32
            )
            s = jnp.where(row == there, one, s)
            lens = jnp.where(row == there, step_lens[seq], lens)
        seen = (lax.rem(lane, 2) == m) & (me * slots + lane // 2 < lens)
        s = jnp.where(seen, s, HIDDEN)
        own = jnp.sum(q * new_keys[m, rows:].astype(jnp.float32)[:1], axis=1, keepdims=True)
        mine = jnp.where(slot == nz - 1, y, EXTRA)
        own = jnp.where(row[:, :1] == mine, own, HIDDEN)
        top = jnp.maximum(jnp.max(s, axis=1, keepdims=True), own)
        w = jnp.exp2((s - top) * fold)
        own_w = jnp.exp2((own - top) * fold)
        total = jnp.sum(w, axis=1, keepdims=True) + own_w
        packed = jnp.dot(
            w.astype(jnp.bfloat16), halves[...], preferred_element_type=jnp.float32
        ).astype(jnp.bfloat16)
        wide_row = lax.broadcasted_iota(jnp.int32, (EXTRA, wide), 0)
        summed = jnp.zeros((EXTRA, wide), jnp.float32)
        for there in range(ny):
            seq = home * ny + there
            at = pl.ds(pl.multiple_of(seq * slots, slots), slots)
            one = jnp.dot(packed, step_v[at, :], preferred_element_type=jnp.float32)
            summed = jnp.where(wide_row == there, one, summed)
        own_w = own_w.astype(jnp.bfloat16).astype(jnp.float32)
        summed = summed + own_w * new_values[rows:].astype(jnp.float32)[:1]
        return top, total, summed

    def join(m, h, slot, top, total, summed):
        at = pl.ds(h * half, half + h * EXTRA)
        old = got_s[m, slot, h]
        places = [(2 * blocks * j, blocks) for j in range(2)] + [(4 * blocks, 2)] * h
        old_top = jnp.concatenate([spread(old, first, n, TILE) for first, n in places], axis=0)
        old_total = jnp.concatenate([spread(old, first + n, n, TILE) for first, n in places], axis=0)
        best = jnp.maximum(old_top, top)
        old_scale = jnp.exp2((old_top - best) * fold)
        new_scale = jnp.exp2((top - best) * fold)
        norm = old_total * old_scale + total * new_scale
        for c in range(0, wide, TILE):
            mixed = got_v[m, slot, at, c : c + TILE].astype(jnp.float32) * old_scale
            mixed = mixed + summed[:, c : c + TILE] * new_scale
            sent_v[m, slot, at, c : c + TILE] = mixed.astype(jnp.bfloat16)
        columns = []
        line = 0
        for first, n in places:
            for i in range(n):
                columns.append((first + i, best[line : line + 8]))
                columns.append((first + n + i, norm[line : line + 8]))
                line += 8
        sent_s[m, slot, h] = pack_columns(columns)

    units = [(m, h) for m in range(2) for h in range(2)]

    def turn_step(slot, carry):
        @pl.when(slot < nz - 2)
        def _():
            fan_out(slot + 1)

        for m in range(2):
            for turn in range(1, ny):
                from_y(m, slot, turn).wait_recv()
        homes = [lax.rem(z + nz - 1 - slot, nz), lax.rem(z + 1 + slot, nz)]
        offs = [[(homes[m] * ny + 2 * h - me) * rows for h in range(2)] for m in range(2)]
        tops = [None] * len(units)
        tops[0] = score(0, 0, slot, offs[0][0])
        for u, (m, h) in enumerate(units):
            if u + 1 < len(units):
                m2, h2 = units[u + 1]
                tops[u + 1] = score(m2, h2, slot, offs[m2][h2])
            top = tops[u]
            summed, total = weigh(m, h, top)
            if h == 1:
                low = decode(m, slot, homes[m])
                top, total, summed = [
                    jnp.concatenate([p, q], axis=0) for p, q in zip((top, total, summed), low)
                ]

            @pl.when(slot > 0)
            def _():
                for copy in ring(m, slot - 1, h):
                    copy.wait_recv()

            join(m, h, slot, top, total, summed)

            @pl.when(slot < nz - 1)
            def _():
                for copy in ring(m, slot, h):
                    copy.start()

            @pl.when(slot == nz - 1)
            def _():
                for there in range(ny):
                    @pl.when(y != there)
                    def _():
                        picks = [0] * (there // 2 == h) + [1, 2] * h
                        for i in picks:
                            final(m, there, i).start()
        return carry

    lax.fori_loop(0, nz, turn_step, 0)

    for m in range(2):
        for turn in range(1, ny):
            for copy in final_from(m, lax.rem(y + turn, ny)):
                copy.wait_recv()
    odd = lax.rem(y, 2) == 1

    def own_half(stats):
        return jnp.where(odd, pltpu.roll(stats, TILE - 2 * blocks, 1), stats)

    def merge(vals, tops, totals):
        best = functools.reduce(jnp.maximum, tops)
        scales = [jnp.exp2((t - best) * fold) for t in tops]
        norm = functools.reduce(jnp.add, [a * b for a, b in zip(scales, totals)])
        total = functools.reduce(jnp.add, [a * b.astype(jnp.float32) for a, b in zip(scales, vals)])
        return total / norm

    peers = [lax.rem(y + turn, ny) for turn in range(1, ny)]
    maps_out = []
    for m in range(2):
        vals = [sent_v[m, nz - 1, deep:]] + [far_d[m, there] for there in peers]
        stats = [sent_s[m, nz - 1, 1]] + [far_s[m, there, 1] for there in peers]
        maps_out.append(
            merge(
                vals,
                [spread(s, 4 * blocks, 2, wide) for s in stats],
                [spread(s, 4 * blocks + 2, 2, wide) for s in stats],
            )
        )
    lines = mix_maps(maps_out[0], maps_out[1], ratio[0, 0], gain[...]).astype(jnp.float32)
    place = lax.broadcasted_iota(jnp.int32, lines.shape, 0)
    line = jnp.sum(jnp.where(place == y, lines, 0.0), axis=0, keepdims=True)
    out[rows:, :] = jnp.where(place == 0, line, 0.0).astype(jnp.bfloat16)

    stats = [
        [own_half(sent_s[m, nz - 1, y // 2])] + [own_half(far_s[m, there, y // 2]) for there in peers]
        for m in range(2)
    ]
    cut = 32
    for j in range(rows // cut):
        maps_out = []
        for m in range(2):
            at = pl.ds(pl.multiple_of(y * rows + j * cut, cut), cut)
            vals = [sent_v[m, nz - 1, at, :]]
            vals += [far_v[m, there, j * cut : (j + 1) * cut, :] for there in peers]
            first = j * cut // 8
            maps_out.append(
                merge(
                    vals,
                    [spread(s, first, cut // 8, wide) for s in stats[m]],
                    [spread(s, blocks + first, cut // 8, wide) for s in stats[m]],
                )
            )
        out[j * cut : (j + 1) * cut, :] = mix_maps(maps_out[0], maps_out[1], ratio[0, 0], gain[...])

    for m in range(2):
        for there in range(ny):
            @pl.when(y != there)
            def _():
                for i in range(3):
                    final(m, there, i).wait_send()
        for turn in range(1, ny):
            along_y(m, nz - 1, turn, q_own.at[m]).wait_send()

    def drain(slot, carry):
        for m in range(2):
            along_z(m, slot).wait_send()
            for turn in range(1, ny):
                along_y(m, slot, turn, q_own.at[m]).wait_send()
            for h in range(2):
                for copy in ring(m, slot, h):
                    copy.wait_send()
        return carry

    lax.fori_loop(0, nz - 1, drain, 0)


def ring_attend(
    ratio, prompt_len, step_lens, gain, queries, new_keys, new_values,
    prompt_keys, prompt_values, cache_keys, cache_values, kv_count, collective,
):
    tall, dims = queries.shape[1:]
    rows = tall - EXTRA
    wide = new_values.shape[1]
    cached = prompt_values.shape[0]
    keys = cached + TILE
    ny = SIDE_Y
    nz = kv_count // ny
    deep = ny * rows + EXTRA
    smem = pl.BlockSpec(memory_space=pltpu.SMEM)
    vmem = pl.BlockSpec(memory_space=pltpu.VMEM)
    far = pl.BlockSpec(memory_space=pl.ANY)
    dma = pltpu.SemaphoreType.DMA
    half = jnp.bfloat16
    fold = dims ** (-0.5) * math.log2(math.e)
    return pl.pallas_call(
        functools.partial(ring_kernel, kv_count, fold),
        out_shape=jax.ShapeDtypeStruct((tall, wide), half),
        in_specs=[smem] * 3 + [vmem] * 4 + [far] * 4,
        out_specs=vmem,
        scratch_shapes=[
            pltpu.VMEM((2, tall, dims), half),
            pltpu.VMEM((2, nz, ny, tall, dims), half),
            pltpu.VMEM(prompt_keys.shape, half),
            pltpu.VMEM((2, dims, keys), half),
            pltpu.VMEM((keys, wide), half),
            pltpu.VMEM((1, cached), jnp.float32),
            pltpu.VMEM((2 * TILE, TILE), half),
            pltpu.VMEM(cache_keys.shape, half),
            pltpu.VMEM(cache_values.shape, half),
            pltpu.VMEM((2, 2 * rows, keys), jnp.float32),
            pltpu.VMEM((2, 2 * rows, keys), half),
            pltpu.VMEM((2, nz, deep, wide), half),
            pltpu.VMEM((2, nz, 2, 8, TILE), jnp.float32),
            pltpu.VMEM((2, nz, deep, wide), half),
            pltpu.VMEM((2, nz, 2, 8, TILE), jnp.float32),
            pltpu.VMEM((2, ny, rows, wide), half),
            pltpu.VMEM((2, ny, 2, 8, TILE), jnp.float32),
            pltpu.VMEM((2, ny, EXTRA, wide), half),
            dma((4,)),
            dma((2, nz)), dma((2, nz)),
            dma((2, nz, ny)), dma((2, nz, ny)),
            dma((2, nz, 2, 2)), dma((2, nz, 2, 2)),
            dma((2, ny, 3)), dma((2, ny, 3)),
        ],
        compiler_params=pltpu.CompilerParams(
            collective_id=collective, has_side_effects=True, vmem_limit_bytes=56 * 1024 * 1024
        ),
        name="ring_attend",
    )(
        ratio, prompt_len, step_lens, gain, queries, new_keys, new_values,
        prompt_keys, prompt_values, cache_keys, cache_values,
    )


def project_out_kernel(axis, count, heads, weight, out, terms, pair, half, far, d_send, d_recv, x_send, x_recv):
    me = lax.axis_index(axis)
    chips = count // 2
    chip, core = me // 2, lax.rem(me, 2)
    meet(axis, count)
    wide = out.shape[1]
    for target in range(count):
        terms[target] = jnp.dot(
            heads[...], weight[:, target * wide : target * wide + wide], preferred_element_type=jnp.float32
        ).astype(jnp.bfloat16)
    near = []
    for turn in range(1, chips + 1):
        there = lax.rem(chip + turn, chips)
        copy = pltpu.make_async_remote_copy(
            src_ref=terms.at[there * 2 + 1 - core],
            dst_ref=pair.at[there],
            send_sem=d_send.at[turn],
            recv_sem=d_recv.at[turn],
            device_id={axis: chip * 2 + 1 - core},
            device_id_type=MESH,
        )
        copy.start()
        near.append(copy)
    away = []
    for turn in range(1, chips + 1):
        near[turn - 1].wait()
        there = lax.rem(chip + turn, chips)
        both = terms[there * 2 + core].astype(jnp.float32) + pair[there].astype(jnp.float32)
        if turn == chips:
            total = both
            for copy in away:
                copy.wait()
            for slot in range(1, chips):
                total = total + far[slot].astype(jnp.float32)
            out[...] = total.astype(jnp.bfloat16)
        else:
            half[turn] = both.astype(jnp.bfloat16)
            copy = pltpu.make_async_remote_copy(
                src_ref=half.at[turn],
                dst_ref=far.at[turn],
                send_sem=x_send.at[turn],
                recv_sem=x_recv.at[turn],
                device_id={axis: there * 2 + core},
                device_id_type=MESH,
            )
            copy.start()
            away.append(copy)


def project_out(heads, weight, axis, count, collective):
    wide = weight.shape[1] // count
    rows = heads.shape[0]
    chips = count // 2
    vmem = pl.BlockSpec(memory_space=pltpu.VMEM)
    return pl.pallas_call(
        functools.partial(project_out_kernel, axis, count),
        out_shape=jax.ShapeDtypeStruct((rows, wide), jnp.bfloat16),
        in_specs=[vmem, vmem],
        out_specs=vmem,
        scratch_shapes=[
            pltpu.VMEM((count, rows, wide), jnp.bfloat16),
            pltpu.VMEM((chips, rows, wide), jnp.bfloat16),
            pltpu.VMEM((chips, rows, wide), jnp.bfloat16),
            pltpu.VMEM((chips, rows, wide), jnp.bfloat16),
            pltpu.SemaphoreType.DMA((chips + 1,)),
            pltpu.SemaphoreType.DMA((chips + 1,)),
            pltpu.SemaphoreType.DMA((chips + 1,)),
            pltpu.SemaphoreType.DMA((chips + 1,)),
        ],
        compiler_params=pltpu.CompilerParams(
            collective_id=collective, has_side_effects=True, vmem_limit_bytes=56 * 1024 * 1024
        ),
        name="project_out",
    )(heads, weight)


def on_device(
    kv_count,
    tp_count,
    piece_tokens,
    step_tokens,
    in_gain,
    w_query,
    w_key,
    w_value,
    w_out,
    mix_ratio,
    out_gain,
    prompt_keys,
    prompt_values,
    step_cache_keys,
    step_cache_values,
    prompt_len,
    step_lens,
):
    piece_dev = piece_tokens.shape[0]
    step_dev = step_tokens.shape[0]
    heads, maps, dims = w_query.shape[1:]
    wide = w_value.shape[-1]
    padded = -(-(piece_dev + step_dev) // EXTRA) * EXTRA
    spare = jnp.zeros((padded - piece_dev - step_dev, piece_tokens.shape[1]), jnp.bfloat16)
    all_rows = jnp.concatenate([piece_tokens, step_tokens, spare], axis=0)
    normed = norm_rows(all_rows, in_gain)
    queries = project(normed, w_query)
    key_rows = project(normed, w_key)
    value_rows = project(normed, w_value)
    end = piece_dev + step_dev

    def rows_of(flat, start, stop, extra):
        return jnp.transpose(flat[:, start:stop], (1, 0, 2)).reshape((stop - start,) + extra)

    piece_k = rows_of(key_rows, 0, piece_dev, (heads, maps, dims))
    step_k = rows_of(key_rows, piece_dev, end, (heads, maps, dims))
    piece_v = rows_of(value_rows, 0, piece_dev, (heads, wide))
    step_v = rows_of(value_rows, piece_dev, end, (heads, wide))
    flat_heads = ring_attend(
        mix_ratio[None, :],
        prompt_len,
        step_lens,
        out_gain[None, :],
        queries,
        key_rows,
        value_rows[0],
        prompt_keys.reshape(-1, dims),
        prompt_values.reshape(-1, wide),
        step_cache_keys.reshape(-1, dims),
        step_cache_values.reshape(-1, wide),
        kv_count,
        1,
    )
    mixed = project_out(flat_heads, w_out.reshape(-1, w_out.shape[-1]), "tp", tp_count, 2)
    return (mixed[:piece_dev], mixed[piece_dev:end], piece_k, piece_v, step_k, step_v)


def solution(mesh):
    in_specs = (
        P("kv", None),
        P("kv", None),
        P(),
        P(None, "tp", None, None),
        P(None, "tp", None, None),
        P(None, "tp", None),
        P("tp", None, None),
        P("tp"),
        P(),
        P("kv", "tp", None, None),
        P("kv", "tp", None),
        P(None, "kv", "tp", None, None),
        P(None, "kv", "tp", None),
        P(),
        P(),
    )
    out_specs = (
        P("kv", "tp"),
        P("kv", "tp"),
        P("kv", "tp", None, None),
        P("kv", "tp", None),
        P("kv", "tp", None, None),
        P("kv", "tp", None),
    )
    return jax.shard_map(
        functools.partial(on_device, mesh.shape["kv"], mesh.shape["tp"]),
        mesh=mesh, in_specs=in_specs, out_specs=out_specs, check_vma=False
    )
```

```python
import functools
import math

import jax
import jax.numpy as jnp
from jax import lax
from jax.experimental import pallas as pl
from jax.experimental.pallas import tpu as pltpu
from jax.sharding import PartitionSpec as P

EPS = 1e-06
OUT_SCALE = 0.8
MESH = pl.DeviceIdType.MESH
HIDDEN = -1e30


def finish_kernel(mixed, line, keys, vals, piece_out, step_out, piece_k, piece_v, step_k, step_v):
    rows = piece_out.shape[0]
    piece_out[...] = mixed[...]
    step_out[...] = line[...]
    piece_v[...] = vals[:rows]
    step_v[...] = vals[rows:].astype(jnp.float32)[:1].astype(jnp.bfloat16)
    up = lax.broadcasted_iota(jnp.int32, (2 * rows, rows), 0)
    right = lax.broadcasted_iota(jnp.int32, (2 * rows, rows), 1)
    total = None
    for m in range(2):
        pick = (up == 2 * right + m).astype(jnp.float32).astype(jnp.bfloat16)
        part = jnp.dot(pick, keys[m, :rows], preferred_element_type=jnp.float32)
        total = part if total is None else total + part
    piece_k[...] = total.astype(jnp.bfloat16)
    both = [keys[m, rows:].astype(jnp.float32)[:1] for m in range(2)]
    step_k[...] = jnp.concatenate(both, axis=0).astype(jnp.bfloat16)


def finish(mixed, line, keys, vals):
    rows, span = mixed.shape
    dims = keys.shape[-1]
    wide = vals.shape[-1]
    vmem = pl.BlockSpec(memory_space=pltpu.VMEM)
    shapes = [(rows, span), (1, span), (2 * rows, dims), (rows, wide), (2, dims), (1, wide)]
    return pl.pallas_call(
        finish_kernel,
        out_shape=[jax.ShapeDtypeStruct(shape, jnp.bfloat16) for shape in shapes],
        in_specs=[vmem] * 4,
        out_specs=[vmem] * 6,
        compiler_params=pltpu.CompilerParams(vmem_limit_bytes=62 * 1024 * 1024),
        name="finish",
    )(mixed, line, keys, vals)


def mix_maps(first, second, ratio, gain):
    mixed = first - ratio * second
    inv_rms = lax.rsqrt(jnp.mean(mixed * mixed, axis=-1, keepdims=True) + EPS)
    return (mixed * inv_rms * gain * OUT_SCALE).astype(jnp.bfloat16)


SIDE_Y = 4
TILE = 128
EXTRA = 16


def spread(stats, first, groups, width):
    cols = [jnp.broadcast_to(stats[:, i : i + 1], (8, width)) for i in range(first, first + groups)]
    return jnp.concatenate(cols, axis=0)


def pack_columns(columns):
    lane = lax.broadcasted_iota(jnp.int32, (8, TILE), 1)
    out = jnp.zeros((8, TILE), jnp.float32)
    for place, column in columns:
        out = jnp.where(lane == place, column, out)
    return out


def ring_kernel(
    kv_count, tp_count, fold, step_lens, ratio, prompt_len, gain,
    piece, step, scale_in, w_query, w_key, w_value,
    prompt_keys, prompt_values, cache_keys, cache_values, w_out, piece_out, step_out, new_keys, new_values,
    tokens, step_token, scales, wq, wk, wv, normed, spaced, both, q_own, q_all, pairs, kt, values, bias, halves, step_k, step_v, scores, weights,
    sent_v, sent_s, got_v, got_s, far_v, far_s, far_d, cols, heads,
    load_sem, qz_send, qz_recv, qy_send, qy_recv, r_send, r_recv, f_send, f_recv,
    c_send, c_recv, h_send, h_recv, d_send, d_recv,
):
    ny = SIDE_Y
    nz = kv_count // ny
    tall, dims = new_keys.shape[1:]
    model = piece.shape[1]
    rows = tall - EXTRA
    wide = values.shape[1]
    cached = bias.shape[1]
    total_keys = values.shape[0]
    slots = step_v.shape[0] // kv_count
    half = 2 * rows
    blocks = rows // 8
    deep = 2 * half
    me = lax.axis_index("kv")
    z = me // ny
    y = lax.rem(me, ny)
    other_z = [lax.rem(z + 1, nz) * ny + y, lax.rem(z + nz - 1, nz) * ny + y]
    mine = lax.axis_index("tp")
    chips = tp_count // 2
    chip = mine // 2
    core = lax.rem(mine, 2)
    span = piece_out.shape[1]

    def load(i, source, target):
        copy = pltpu.make_async_copy(source, target, load_sem.at[i])
        copy.start()
        return copy

    first_loads = [
        load(0, piece, tokens.at[pl.ds(0, rows)]),
        load(1, step, step_token),
        load(2, scale_in, scales),
    ]
    wq_load = load(3, w_query, wq)
    wk_load = load(4, w_key, wk)
    pairs_load = load(5, prompt_keys, pairs)
    wv_load = load(6, w_value, wv)
    last_loads = [
        load(7, prompt_values, values.at[pl.ds(0, cached)]),
        load(8, cache_keys, step_k),
        load(9, cache_values, step_v),
        load(10, w_out.at[:, pl.ds(pl.multiple_of(mine * span, span), span)], cols.at[mine]),
    ]

    barrier = pltpu.get_barrier_semaphore()
    for there in other_z + [z * ny + lax.rem(y + turn, ny) for turn in range(1, ny)]:
        pl.semaphore_signal(barrier, inc=1, device_id={"kv": there}, device_id_type=MESH)
    for turn in range(1, tp_count):
        there = lax.rem(mine + turn, tp_count)
        pl.semaphore_signal(barrier, inc=1, device_id={"tp": there}, device_id_type=MESH)

    for m in range(2):
        got_v[m, 0] = jnp.zeros(got_v.shape[2:], jnp.bfloat16)
        lane = lax.broadcasted_iota(jnp.int32, (8, TILE), 1)
        spot = jnp.where(lane < 4 * blocks, lax.rem(lane, 2 * blocks), lane - 4 * blocks + blocks - 2)
        for h in range(2):
            got_s[m, 0, h] = jnp.where(spot < blocks, HIDDEN, 0.0)
    up = lax.broadcasted_iota(jnp.int32, (TILE, 4 * TILE), 0)
    right = lax.broadcasted_iota(jnp.int32, (TILE, 4 * TILE), 1)
    gap = jnp.where(right < 2 * TILE, 2 * up, 2 * up + 2 * TILE + 1)
    open_up = (gap == right).astype(jnp.float32).astype(jnp.bfloat16)

    for copy in first_loads:
        copy.wait()
    place = lax.broadcasted_iota(jnp.int32, (EXTRA, model), 0)
    low = jnp.broadcast_to(step_token[...].astype(jnp.float32), (EXTRA, model))
    tokens[rows:] = jnp.where(place == 0, low, 0.0).astype(jnp.bfloat16)

    def norm(i, carry):
        at = pl.ds(pl.multiple_of(i * EXTRA, EXTRA), EXTRA)
        floats = tokens[at, :].astype(jnp.float32)
        inv_rms = lax.rsqrt(jnp.mean(floats * floats, axis=-1, keepdims=True) + EPS)
        normed[at, :] = (floats * inv_rms * scales[...]).astype(jnp.bfloat16)
        return carry

    lax.fori_loop(0, tall // EXTRA, norm, 0)
    for i in range(model // TILE):
        wider = jnp.dot(normed[:, i * TILE : (i + 1) * TILE], open_up, preferred_element_type=jnp.float32)
        for m in range(2):
            part = wider[:, m * 2 * TILE : (m + 1) * 2 * TILE]
            spaced[m * tall : (m + 1) * tall, i * 2 * TILE : (i + 1) * 2 * TILE] = part.astype(jnp.bfloat16)
    wq_load.wait()
    both[...] = jnp.dot(spaced[...], wq[...], preferred_element_type=jnp.float32).astype(jnp.bfloat16)
    extra_row = lax.broadcasted_iota(jnp.int32, (EXTRA, dims), 0)
    for m in range(2):
        q_own[m, :rows] = both[m * tall : m * tall + rows]
        line = both[m * tall + rows : (m + 1) * tall].astype(jnp.float32)[:1]
        q_own[m, rows:] = jnp.where(extra_row == y, line, 0.0).astype(jnp.bfloat16)
        q_all[m, nz - 1, y] = q_own[m]

    def to(src, dst, send, recv, device):
        return pltpu.make_async_remote_copy(
            src_ref=src, dst_ref=dst, send_sem=send, recv_sem=recv,
            device_id={"kv": device}, device_id_type=MESH,
        )

    def across(src, dst, send, recv, device):
        return pltpu.make_async_remote_copy(
            src_ref=src, dst_ref=dst, send_sem=send, recv_sem=recv,
            device_id={"tp": device}, device_id_type=MESH,
        )

    def along_z(m, slot, source):
        return to(source, q_all.at[m, slot, y], qz_send.at[m, slot], qz_recv.at[m, slot], other_z[m])

    def along_y(m, slot, turn, source):
        return to(
            source, q_all.at[m, slot, y], qy_send.at[m, slot, turn], qy_recv.at[m, slot, y],
            z * ny + lax.rem(y + turn, ny),
        )

    def from_y(m, slot, turn):
        there = lax.rem(y + turn, ny)
        return to(
            q_all.at[m, slot, there], q_all.at[m, slot, there],
            qy_send.at[m, slot, turn], qy_recv.at[m, slot, there], z * ny + there,
        )

    def ring(m, slot, h):
        at = pl.ds(h * half, half + h * EXTRA)
        return (
            to(sent_s.at[m, slot, h], got_s.at[m, slot + 1, h],
               r_send.at[m, slot, h, 0], r_recv.at[m, slot, h, 0], other_z[m]),
            to(sent_v.at[m, slot, at], got_v.at[m, slot + 1, at],
               r_send.at[m, slot, h, 1], r_recv.at[m, slot, h, 1], other_z[m]),
        )

    def final(m, there, i):
        at = pl.ds(pl.multiple_of(there * rows, 32), rows)
        low = pl.ds(deep, EXTRA)
        peer = z * ny + there
        src = (sent_v.at[m, nz - 1, at], sent_s.at[m, nz - 1], sent_v.at[m, nz - 1, low])[i]
        dst = (far_v, far_s, far_d)[i].at[m, y]
        return to(src, dst, f_send.at[m, there, i], f_recv.at[m, y, i], peer)

    def final_from(m, there):
        peer = z * ny + there
        return tuple(
            to(ref.at[m, there], ref.at[m, there], f_send.at[m, there, i], f_recv.at[m, there, i], peer)
            for i, ref in enumerate((far_v, far_s, far_d))
        )

    pl.semaphore_wait(barrier, ny + tp_count)
    for m in range(2):
        along_z(m, 0, q_own.at[m]).start()

    def columns_to(turn):
        there = lax.rem(mine + turn, tp_count)
        return across(
            w_out.at[:, pl.ds(pl.multiple_of(there * span, span), span)], cols.at[mine],
            c_send.at[turn], c_recv.at[turn], there,
        )

    def pass_on(slot):
        for m in range(2):
            along_z(m, slot, q_own.at[m]).wait_recv()

            @pl.when(slot < nz - 2)
            def _():
                along_z(m, slot + 1, q_all.at[m, slot, y]).start()

            for turn in range(1, ny):
                along_y(m, slot, turn, q_all.at[m, slot, y]).start()

    up = lax.broadcasted_iota(jnp.int32, (2 * TILE, 2 * TILE), 0)
    right = lax.broadcasted_iota(jnp.int32, (2 * TILE, 2 * TILE), 1)
    sort = jnp.where(right < TILE, 2 * right, 2 * right - 2 * TILE + 1) == up
    sort = sort.astype(jnp.float32).astype(jnp.bfloat16)

    def split(i, carry):
        block = pairs[pl.ds(pl.multiple_of(i * 2 * TILE, 2 * TILE), 2 * TILE), :]
        turned = lax.dot_general(
            block, sort, (((0,), (0,)), ((), ())), preferred_element_type=jnp.float32
        ).astype(jnp.bfloat16)
        at = pl.ds(pl.multiple_of(i * TILE, TILE), TILE)
        kt[0, :, at] = turned[:, :TILE]
        kt[1, :, at] = turned[:, TILE:]
        return carry

    wk_load.wait()
    made = jnp.dot(spaced[...], wk[...], preferred_element_type=jnp.float32).astype(jnp.bfloat16)
    for m in range(2):
        new_keys[m] = made[m * tall : (m + 1) * tall]
    pairs_load.wait()
    lax.fori_loop(0, cached // TILE // 2, split, 0)
    pass_on(0)
    wv_load.wait()
    new_values[...] = jnp.dot(normed[...], wv[...], preferred_element_type=jnp.float32).astype(jnp.bfloat16)
    lax.fori_loop(cached // TILE // 2, cached // TILE, split, 0)
    pass_on(1)
    for turn in range(1, tp_count):
        columns_to(turn).start()
    key_lane = lax.broadcasted_iota(jnp.int32, (1, cached), 1)
    bias[...] = jnp.where(me * cached + key_lane < prompt_len[...], 0.0, HIDDEN)
    values[cached : cached + rows] = new_values[:rows]
    values[cached + rows :] = jnp.zeros((total_keys - cached - rows, wide), jnp.bfloat16)
    for m in range(2):
        fresh = jnp.concatenate(
            [new_keys[m, :rows].astype(jnp.float32), jnp.zeros((TILE - rows, dims), jnp.float32)], axis=0
        )
        kt[m, :, cached:] = jnp.transpose(fresh).astype(jnp.bfloat16)
    up = lax.broadcasted_iota(jnp.int32, (2 * TILE, TILE), 0)
    right = lax.broadcasted_iota(jnp.int32, (2 * TILE, TILE), 1)
    halves[...] = (up // 2 == right).astype(jnp.float32).astype(jnp.bfloat16)
    for copy in last_loads:
        copy.wait()

    def score(m, h, slot, off):
        q = q_all[m, slot, 2 * h : 2 * h + 2, :rows].reshape(half, dims)
        buf = (2 * m + h) % 2
        best = None
        for c in range(0, cached, 256):
            s = jnp.dot(q, kt[m, :, c : c + 256], preferred_element_type=jnp.float32)
            s = s + bias[:, c : c + 256]
            scores[buf, :, c : c + 256] = s
            for j in range(0, 256, TILE):
                p = s[:, j : j + TILE]
                best = p if best is None else jnp.maximum(best, p)
        tail = jnp.dot(q, kt[m, :, cached:], preferred_element_type=jnp.float32)
        lane = lax.broadcasted_iota(jnp.int32, tail.shape, 1)
        row = lax.broadcasted_iota(jnp.int32, tail.shape, 0)
        gap = jnp.where(lane < rows, lane - row, 1 << 20)
        tail = jnp.where(gap <= off, tail, HIDDEN)
        scores[buf, :, cached:] = tail
        best = jnp.maximum(best, tail)
        return jnp.max(best, axis=1, keepdims=True)

    def weigh(m, h, top):
        buf = (2 * m + h) % 2
        part = None
        for c in range(0, total_keys, TILE):
            w = jnp.exp2((scores[buf, :, c : c + TILE] - top) * fold)
            weights[buf, :, c : c + TILE] = w.astype(jnp.bfloat16)
            part = w if part is None else part + w
        total = jnp.sum(part, axis=1, keepdims=True)
        return jnp.dot(weights[buf], values[...], preferred_element_type=jnp.float32), total

    def decode(m, slot, home):
        q = q_all[m, slot, 0, rows:].astype(jnp.float32)
        for there in range(1, ny):
            q = q + q_all[m, slot, there, rows:].astype(jnp.float32)
        qb = q.astype(jnp.bfloat16)
        row = lax.broadcasted_iota(jnp.int32, (EXTRA, 2 * slots), 0)
        lane = lax.broadcasted_iota(jnp.int32, (EXTRA, 2 * slots), 1)
        s = jnp.zeros((EXTRA, 2 * slots), jnp.float32)
        lens = jnp.zeros((EXTRA, 2 * slots), jnp.int32)
        for there in range(ny):
            seq = home * ny + there
            at = pl.ds(pl.multiple_of(seq * 2 * slots, 2 * slots), 2 * slots)
            one = lax.dot_general(
                qb, step_k[at, :], (((1,), (1,)), ((), ())), preferred_element_type=jnp.float32
            )
            s = jnp.where(row == there, one, s)
            lens = jnp.where(row == there, step_lens[seq], lens)
        seen = (lax.rem(lane, 2) == m) & (me * slots + lane // 2 < lens)
        s = jnp.where(seen, s, HIDDEN)
        own = jnp.sum(q * new_keys[m, rows:].astype(jnp.float32)[:1], axis=1, keepdims=True)
        mine = jnp.where(slot == nz - 1, y, EXTRA)
        own = jnp.where(row[:, :1] == mine, own, HIDDEN)
        top = jnp.maximum(jnp.max(s, axis=1, keepdims=True), own)
        w = jnp.exp2((s - top) * fold)
        own_w = jnp.exp2((own - top) * fold)
        total = jnp.sum(w, axis=1, keepdims=True) + own_w
        packed = jnp.dot(
            w.astype(jnp.bfloat16), halves[...], preferred_element_type=jnp.float32
        ).astype(jnp.bfloat16)
        wide_row = lax.broadcasted_iota(jnp.int32, (EXTRA, wide), 0)
        summed = jnp.zeros((EXTRA, wide), jnp.float32)
        for there in range(ny):
            seq = home * ny + there
            at = pl.ds(pl.multiple_of(seq * slots, slots), slots)
            one = jnp.dot(packed, step_v[at, :], preferred_element_type=jnp.float32)
            summed = jnp.where(wide_row == there, one, summed)
        own_w = own_w.astype(jnp.bfloat16).astype(jnp.float32)
        summed = summed + own_w * new_values[rows:].astype(jnp.float32)[:1]
        return top, total, summed

    def join(m, h, slot, top, total, summed):
        at = pl.ds(h * half, half + h * EXTRA)
        old = got_s[m, slot, h]
        places = [(2 * blocks * j, blocks) for j in range(2)] + [(4 * blocks, 2)] * h
        old_top = jnp.concatenate([spread(old, first, n, TILE) for first, n in places], axis=0)
        old_total = jnp.concatenate([spread(old, first + n, n, TILE) for first, n in places], axis=0)
        best = jnp.maximum(old_top, top)
        old_scale = jnp.exp2((old_top - best) * fold)
        new_scale = jnp.exp2((top - best) * fold)
        norm = old_total * old_scale + total * new_scale
        for c in range(0, wide, TILE):
            mixed = got_v[m, slot, at, c : c + TILE].astype(jnp.float32) * old_scale
            mixed = mixed + summed[:, c : c + TILE] * new_scale
            sent_v[m, slot, at, c : c + TILE] = mixed.astype(jnp.bfloat16)
        columns = []
        line = 0
        for first, n in places:
            for i in range(n):
                columns.append((first + i, best[line : line + 8]))
                columns.append((first + n + i, norm[line : line + 8]))
                line += 8
        sent_s[m, slot, h] = pack_columns(columns)

    units = [(m, h) for m in range(2) for h in range(2)]

    def turn_step(slot, carry):
        for turn in range(1, ny):
            from_y(0, slot, turn).wait_recv()
        homes = [lax.rem(z + nz - 1 - slot, nz), lax.rem(z + 1 + slot, nz)]
        offs = [[(homes[m] * ny + 2 * h - me) * rows for h in range(2)] for m in range(2)]
        tops = [None] * len(units)
        tops[0] = score(0, 0, slot, offs[0][0])
        for u, (m, h) in enumerate(units):
            if u == 1:
                for turn in range(1, ny):
                    from_y(1, slot, turn).wait_recv()
            if u + 1 < len(units):
                m2, h2 = units[u + 1]
                tops[u + 1] = score(m2, h2, slot, offs[m2][h2])
            top = tops[u]
            summed, total = weigh(m, h, top)
            if h == 1:
                low = decode(m, slot, homes[m])
                top, total, summed = [
                    jnp.concatenate([p, q], axis=0) for p, q in zip((top, total, summed), low)
                ]

            @pl.when(slot > 0)
            def _():
                for copy in ring(m, slot - 1, h):
                    copy.wait_recv()

            join(m, h, slot, top, total, summed)

            @pl.when(slot < nz - 1)
            def _():
                for copy in ring(m, slot, h):
                    copy.start()

            if u == 1:
                @pl.when(slot < nz - 3)
                def _():
                    pass_on(slot + 2)

                @pl.when(slot == nz - 3)
                def _():
                    for m2 in range(2):
                        for turn in range(1, ny):
                            along_y(m2, nz - 1, turn, q_own.at[m2]).start()

            @pl.when(slot == nz - 1)
            def _():
                for there in range(ny):
                    @pl.when(y != there)
                    def _():
                        picks = [0] * (there // 2 == h) + [1, 2] * h
                        for i in picks:
                            final(m, there, i).start()
        return carry

    lax.fori_loop(0, nz, turn_step, 0)

    for m in range(2):
        for turn in range(1, ny):
            for copy in final_from(m, lax.rem(y + turn, ny)):
                copy.wait_recv()
    odd = lax.rem(y, 2) == 1

    def own_half(stats):
        return jnp.where(odd, pltpu.roll(stats, TILE - 2 * blocks, 1), stats)

    def merge(vals, tops, totals):
        best = functools.reduce(jnp.maximum, tops)
        scales = [jnp.exp2((t - best) * fold) for t in tops]
        norm = functools.reduce(jnp.add, [a * b for a, b in zip(scales, totals)])
        total = functools.reduce(jnp.add, [a * b.astype(jnp.float32) for a, b in zip(scales, vals)])
        return total / norm

    peers = [lax.rem(y + turn, ny) for turn in range(1, ny)]
    maps_out = []
    for m in range(2):
        vals = [sent_v[m, nz - 1, deep:]] + [far_d[m, there] for there in peers]
        stats = [sent_s[m, nz - 1, 1]] + [far_s[m, there, 1] for there in peers]
        maps_out.append(
            merge(
                vals,
                [spread(s, 4 * blocks, 2, wide) for s in stats],
                [spread(s, 4 * blocks + 2, 2, wide) for s in stats],
            )
        )
    lines = mix_maps(maps_out[0], maps_out[1], ratio[...], gain[...]).astype(jnp.float32)
    place = lax.broadcasted_iota(jnp.int32, lines.shape, 0)
    line = jnp.sum(jnp.where(place == y, lines, 0.0), axis=0, keepdims=True)
    heads[mine, rows:] = jnp.where(place == 0, line, 0.0).astype(jnp.bfloat16)

    stats = [
        [own_half(sent_s[m, nz - 1, y // 2])] + [own_half(far_s[m, there, y // 2]) for there in peers]
        for m in range(2)
    ]
    cut = 32
    for j in range(rows // cut):
        maps_out = []
        for m in range(2):
            at = pl.ds(pl.multiple_of(y * rows + j * cut, cut), cut)
            vals = [sent_v[m, nz - 1, at, :]]
            vals += [far_v[m, there, j * cut : (j + 1) * cut, :] for there in peers]
            first = j * cut // 8
            maps_out.append(
                merge(
                    vals,
                    [spread(s, first, cut // 8, wide) for s in stats[m]],
                    [spread(s, blocks + first, cut // 8, wide) for s in stats[m]],
                )
            )
        heads[mine, j * cut : (j + 1) * cut] = mix_maps(maps_out[0], maps_out[1], ratio[...], gain[...])

    def heads_to(turn):
        there = lax.rem(chip + turn, chips) * 2 + core
        return across(heads.at[mine], heads.at[mine], h_send.at[turn], h_recv.at[turn], there)

    def heads_over(turn):
        whose = lax.rem(chip + chips - turn, chips) * 2 + core
        return across(
            heads.at[whose], heads.at[whose], d_send.at[turn], d_recv.at[turn], chip * 2 + 1 - core
        )

    for turn in (2, 1, 3):
        heads_to(turn).start()
    heads_over(0).start()

    for m in range(2):
        for there in range(ny):
            @pl.when(y != there)
            def _():
                for i in range(3):
                    final(m, there, i).wait_send()
        for turn in range(1, ny):
            along_y(m, nz - 1, turn, q_own.at[m]).wait_send()

    def drain(slot, carry):
        for m in range(2):
            along_z(m, slot, q_own.at[m]).wait_send()
            for turn in range(1, ny):
                along_y(m, slot, turn, q_own.at[m]).wait_send()
            for h in range(2):
                for copy in ring(m, slot, h):
                    copy.wait_send()
        return carry

    lax.fori_loop(0, nz - 1, drain, 0)
    for turn in range(1, tp_count):
        columns_to(turn).wait()

    def term(whose):
        return jnp.dot(heads[whose], cols[whose], preferred_element_type=jnp.float32)

    total = term(mine)
    heads_over(0).wait_recv()
    total = total + term(chip * 2 + 1 - core)
    for turn in (1, 3, 2):
        heads_to(turn).wait_recv()
        heads_over(turn).start()
        total = total + term(lax.rem(chip + chips - turn, chips) * 2 + core)
    for turn in (1, 3, 2):
        heads_over(turn).wait_recv()
        total = total + term(lax.rem(chip + chips - turn, chips) * 2 + 1 - core)
    piece_out[...] = total[:rows].astype(jnp.bfloat16)
    step_out[...] = total[rows:][:1].astype(jnp.bfloat16)
    for turn in range(chips):
        if turn > 0:
            heads_to(turn).wait_send()
        heads_over(turn).wait_send()


def ring_attend(
    step_lens, ratio, prompt_len, gain, piece, step, scale_in, w_query, w_key, w_value,
    prompt_keys, prompt_values, cache_keys, cache_values, w_out, kv_count, tp_count, collective,
):
    rows, model = piece.shape
    tall = rows + EXTRA
    dims = w_query.shape[1]
    wide = w_value.shape[1]
    cached = prompt_values.shape[0]
    keys = cached + TILE
    ny = SIDE_Y
    nz = kv_count // ny
    deep = ny * rows + EXTRA
    span = w_out.shape[1] // tp_count
    smem = pl.BlockSpec(memory_space=pltpu.SMEM)
    vmem = pl.BlockSpec(memory_space=pltpu.VMEM)
    far = pl.BlockSpec(memory_space=pltpu.MemorySpace.HBM)
    dma = pltpu.SemaphoreType.DMA
    half = jnp.bfloat16
    fold = dims ** (-0.5) * math.log2(math.e)
    return pl.pallas_call(
        functools.partial(ring_kernel, kv_count, tp_count, fold),
        out_shape=[
            jax.ShapeDtypeStruct((rows, span), half),
            jax.ShapeDtypeStruct((1, span), half),
            jax.ShapeDtypeStruct((2, tall, dims), half),
            jax.ShapeDtypeStruct((tall, wide), half),
        ],
        in_specs=[smem] + [vmem] * 3 + [far] * 11,
        out_specs=[vmem] * 4,
        scratch_shapes=[
            pltpu.VMEM((tall, model), half),
            pltpu.VMEM(step.shape, half),
            pltpu.VMEM(scale_in.shape, jnp.float32),
            pltpu.VMEM(w_query.shape, half),
            pltpu.VMEM(w_key.shape, half),
            pltpu.VMEM(w_value.shape, half),
            pltpu.VMEM((tall, model), half),
            pltpu.VMEM((2 * tall, 2 * model), half),
            pltpu.VMEM((2 * tall, dims), half),
            pltpu.VMEM((2, tall, dims), half),
            pltpu.VMEM((2, nz, ny, tall, dims), half),
            pltpu.VMEM(prompt_keys.shape, half),
            pltpu.VMEM((2, dims, keys), half),
            pltpu.VMEM((keys, wide), half),
            pltpu.VMEM((1, cached), jnp.float32),
            pltpu.VMEM((2 * TILE, TILE), half),
            pltpu.VMEM(cache_keys.shape, half),
            pltpu.VMEM(cache_values.shape, half),
            pltpu.VMEM((2, 2 * rows, keys), jnp.float32),
            pltpu.VMEM((2, 2 * rows, keys), half),
            pltpu.VMEM((2, nz, deep, wide), half),
            pltpu.VMEM((2, nz, 2, 8, TILE), jnp.float32),
            pltpu.VMEM((2, nz, deep, wide), half),
            pltpu.VMEM((2, nz, 2, 8, TILE), jnp.float32),
            pltpu.VMEM((2, ny, rows, wide), half),
            pltpu.VMEM((2, ny, 2, 8, TILE), jnp.float32),
            pltpu.VMEM((2, ny, EXTRA, wide), half),
            pltpu.VMEM((tp_count, wide, span), half),
            pltpu.VMEM((tp_count, tall, wide), half),
            dma((11,)),
            dma((2, nz)), dma((2, nz)),
            dma((2, nz, ny)), dma((2, nz, ny)),
            dma((2, nz, 2, 2)), dma((2, nz, 2, 2)),
            dma((2, ny, 3)), dma((2, ny, 3)),
            dma((tp_count,)), dma((tp_count,)),
            dma((tp_count // 2,)), dma((tp_count // 2,)),
            dma((tp_count // 2,)), dma((tp_count // 2,)),
        ],
        compiler_params=pltpu.CompilerParams(
            collective_id=collective, has_side_effects=True, vmem_limit_bytes=62 * 1024 * 1024
        ),
        name="ring_attend",
    )(
        step_lens, ratio, prompt_len, gain, piece, step, scale_in, w_query, w_key, w_value,
        prompt_keys, prompt_values, cache_keys, cache_values, w_out,
    )


def on_device(
    kv_count,
    tp_count,
    piece_tokens,
    step_tokens,
    in_gain,
    w_query,
    w_key,
    w_value,
    w_out,
    mix_ratio,
    out_gain,
    prompt_keys,
    prompt_values,
    step_cache_keys,
    step_cache_values,
    prompt_len,
    step_lens,
):
    piece_dev = piece_tokens.shape[0]
    step_dev = step_tokens.shape[0]
    heads, maps, dims = w_query.shape[1:]
    wide = w_value.shape[-1]
    mixed, line, key_rows, value_rows = ring_attend(
        step_lens,
        mix_ratio[None, :],
        prompt_len[None, :],
        out_gain[None, :],
        piece_tokens,
        step_tokens,
        in_gain[None, :],
        w_query.reshape(-1, dims),
        w_key.reshape(-1, dims),
        w_value.reshape(-1, wide),
        prompt_keys.reshape(-1, dims),
        prompt_values.reshape(-1, wide),
        step_cache_keys.reshape(-1, dims),
        step_cache_values.reshape(-1, wide),
        w_out.reshape(-1, w_out.shape[-1]),
        kv_count,
        tp_count,
        0,
    )
    piece_out, step_out, piece_k, piece_v, step_k, step_v = finish(mixed, line, key_rows, value_rows)
    return (
        piece_out,
        step_out,
        piece_k.reshape(piece_dev, heads, maps, dims),
        piece_v.reshape(piece_dev, heads, wide),
        step_k.reshape(step_dev, heads, maps, dims),
        step_v.reshape(step_dev, heads, wide),
    )


def solution(mesh):
    in_specs = (
        P("kv", None),
        P("kv", None),
        P(),
        P(None, "tp", None, None),
        P(None, "tp", None, None),
        P(None, "tp", None),
        P("tp", None, None),
        P("tp"),
        P(),
        P("kv", "tp", None, None),
        P("kv", "tp", None),
        P(None, "kv", "tp", None, None),
        P(None, "kv", "tp", None),
        P(),
        P(),
    )
    out_specs = (
        P("kv", "tp"),
        P("kv", "tp"),
        P("kv", "tp", None, None),
        P("kv", "tp", None),
        P("kv", "tp", None, None),
        P("kv", "tp", None),
    )
    return jax.shard_map(
        functools.partial(on_device, mesh.shape["kv"], mesh.shape["tp"]),
        mesh=mesh, in_specs=in_specs, out_specs=out_specs, check_vma=False
    )
```

```python
import functools
import math

import jax
import jax.numpy as jnp
from jax import lax
from jax.experimental import pallas as pl
from jax.experimental.pallas import tpu as pltpu
from jax.sharding import PartitionSpec as P

EPS = 1e-06
OUT_SCALE = 0.8
MESH = pl.DeviceIdType.MESH
HIDDEN = -1e30


def finish_kernel(mixed, line, keys, vals, piece_out, step_out, piece_k, piece_v, step_k, step_v):
    rows = piece_out.shape[0]
    piece_out[...] = mixed[...]
    step_out[...] = line[...]
    piece_v[...] = vals[:rows]
    step_v[...] = vals[rows:].astype(jnp.float32)[:1].astype(jnp.bfloat16)
    up = lax.broadcasted_iota(jnp.int32, (2 * rows, rows), 0)
    right = lax.broadcasted_iota(jnp.int32, (2 * rows, rows), 1)
    total = None
    for m in range(2):
        pick = (up == 2 * right + m).astype(jnp.float32).astype(jnp.bfloat16)
        part = jnp.dot(pick, keys[m, :rows], preferred_element_type=jnp.float32)
        total = part if total is None else total + part
    piece_k[...] = total.astype(jnp.bfloat16)
    both = [keys[m, rows:].astype(jnp.float32)[:1] for m in range(2)]
    step_k[...] = jnp.concatenate(both, axis=0).astype(jnp.bfloat16)


def finish(mixed, line, keys, vals):
    rows, span = mixed.shape
    dims = keys.shape[-1]
    wide = vals.shape[-1]
    vmem = pl.BlockSpec(memory_space=pltpu.VMEM)
    shapes = [(rows, span), (1, span), (2 * rows, dims), (rows, wide), (2, dims), (1, wide)]
    return pl.pallas_call(
        finish_kernel,
        out_shape=[jax.ShapeDtypeStruct(shape, jnp.bfloat16) for shape in shapes],
        in_specs=[vmem] * 4,
        out_specs=[vmem] * 6,
        compiler_params=pltpu.CompilerParams(vmem_limit_bytes=62 * 1024 * 1024),
        name="finish",
    )(mixed, line, keys, vals)


def mix_maps(first, second, ratio, gain):
    mixed = first - ratio * second
    inv_rms = lax.rsqrt(jnp.mean(mixed * mixed, axis=-1, keepdims=True) + EPS)
    return (mixed * inv_rms * gain * OUT_SCALE).astype(jnp.bfloat16)


SIDE_Y = 4
TILE = 128
EXTRA = 16


def spread(stats, first, groups, width):
    cols = [jnp.broadcast_to(stats[:, i : i + 1], (8, width)) for i in range(first, first + groups)]
    return jnp.concatenate(cols, axis=0)


def pack_columns(columns):
    lane = lax.broadcasted_iota(jnp.int32, (8, TILE), 1)
    out = jnp.zeros((8, TILE), jnp.float32)
    for place, column in columns:
        out = jnp.where(lane == place, column, out)
    return out


def ring_kernel(
    kv_count, tp_count, fold, step_lens, ratio, prompt_len, gain,
    piece, step, scale_in, w_query, w_key, w_value,
    prompt_keys, prompt_values, cache_keys, cache_values, w_out, piece_out, step_out, new_keys, new_values,
    tokens, step_token, scales, wq, wk, wv, normed, spaced, both, q_own, q_all, pairs, kt, values, bias, halves, step_k, step_v, scores, weights,
    sent_v, sent_s, got_v, got_s, far_v, far_s, far_d, cols, heads,
    load_sem, qz_send, qz_recv, qy_send, qy_recv, r_send, r_recv, f_send, f_recv,
    c_send, c_recv, h_send, h_recv, d_send, d_recv,
):
    ny = SIDE_Y
    nz = kv_count // ny
    tall, dims = new_keys.shape[1:]
    model = piece.shape[1]
    rows = tall - EXTRA
    wide = values.shape[1]
    cached = bias.shape[1]
    total_keys = values.shape[0]
    slots = step_v.shape[0] // kv_count
    half = 2 * rows
    blocks = rows // 8
    deep = 2 * half
    me = lax.axis_index("kv")
    z = me // ny
    y = lax.rem(me, ny)
    other_z = [lax.rem(z + 1, nz) * ny + y, lax.rem(z + nz - 1, nz) * ny + y]
    mine = lax.axis_index("tp")
    chips = tp_count // 2
    chip = mine // 2
    core = lax.rem(mine, 2)
    span = piece_out.shape[1]

    def load(i, source, target):
        copy = pltpu.make_async_copy(source, target, load_sem.at[i])
        copy.start()
        return copy

    first_loads = [
        load(0, piece, tokens.at[pl.ds(0, rows)]),
        load(1, step, step_token),
        load(2, scale_in, scales),
    ]
    wq_load = load(3, w_query, wq)
    wk_load = load(4, w_key, wk)
    pairs_load = load(5, prompt_keys, pairs)
    wv_load = load(6, w_value, wv)
    last_loads = [
        load(7, prompt_values, values.at[pl.ds(0, cached)]),
        load(8, cache_keys, step_k),
        load(9, cache_values, step_v),
        load(10, w_out.at[:, pl.ds(pl.multiple_of(mine * span, span), span)], cols.at[mine]),
    ]

    barrier = pltpu.get_barrier_semaphore()
    sides = [lax.rem(z + 1, nz) * ny, lax.rem(z + nz - 1, nz) * ny]
    for side in sides + [z * ny]:
        for turn in range(side is not sides[0] and side is not sides[1], ny):
            there = side + lax.rem(y + turn, ny)
            pl.semaphore_signal(barrier, inc=1, device_id={"kv": there}, device_id_type=MESH)
    for turn in range(1, tp_count):
        there = lax.rem(mine + turn, tp_count)
        pl.semaphore_signal(barrier, inc=1, device_id={"tp": there}, device_id_type=MESH)

    for m in range(2):
        got_v[m, 0] = jnp.zeros(got_v.shape[2:], jnp.bfloat16)
        lane = lax.broadcasted_iota(jnp.int32, (8, TILE), 1)
        spot = jnp.where(lane < 4 * blocks, lax.rem(lane, 2 * blocks), lane - 4 * blocks + blocks - 2)
        for h in range(2):
            got_s[m, 0, h] = jnp.where(spot < blocks, HIDDEN, 0.0)
    up = lax.broadcasted_iota(jnp.int32, (TILE, 4 * TILE), 0)
    right = lax.broadcasted_iota(jnp.int32, (TILE, 4 * TILE), 1)
    gap = jnp.where(right < 2 * TILE, 2 * up, 2 * up + 2 * TILE + 1)
    open_up = (gap == right).astype(jnp.float32).astype(jnp.bfloat16)

    for copy in first_loads:
        copy.wait()
    place = lax.broadcasted_iota(jnp.int32, (EXTRA, model), 0)
    low = jnp.broadcast_to(step_token[...].astype(jnp.float32), (EXTRA, model))
    tokens[rows:] = jnp.where(place == 0, low, 0.0).astype(jnp.bfloat16)

    def norm(i, carry):
        at = pl.ds(pl.multiple_of(i * EXTRA, EXTRA), EXTRA)
        floats = tokens[at, :].astype(jnp.float32)
        inv_rms = lax.rsqrt(jnp.mean(floats * floats, axis=-1, keepdims=True) + EPS)
        normed[at, :] = (floats * inv_rms * scales[...]).astype(jnp.bfloat16)
        return carry

    lax.fori_loop(0, tall // EXTRA, norm, 0)
    for i in range(model // TILE):
        wider = jnp.dot(normed[:, i * TILE : (i + 1) * TILE], open_up, preferred_element_type=jnp.float32)
        for m in range(2):
            slab = wider[:, m * 2 * TILE : (m + 1) * 2 * TILE]
            spaced[m * tall : (m + 1) * tall, i * 2 * TILE : (i + 1) * 2 * TILE] = slab.astype(jnp.bfloat16)
    wq_load.wait()
    both[...] = jnp.dot(spaced[...], wq[...], preferred_element_type=jnp.float32).astype(jnp.bfloat16)
    extra_row = lax.broadcasted_iota(jnp.int32, (EXTRA, dims), 0)
    for m in range(2):
        q_own[m, :rows] = both[m * tall : m * tall + rows]
        line = both[m * tall + rows : (m + 1) * tall].astype(jnp.float32)[:1]
        q_own[m, rows:] = jnp.where(extra_row == y, line, 0.0).astype(jnp.bfloat16)
        q_all[m, nz - 1, y] = q_own[m]

    def to(src, dst, send, recv, device):
        return pltpu.make_async_remote_copy(
            src_ref=src, dst_ref=dst, send_sem=send, recv_sem=recv,
            device_id={"kv": device}, device_id_type=MESH,
        )

    def across(src, dst, send, recv, device):
        return pltpu.make_async_remote_copy(
            src_ref=src, dst_ref=dst, send_sem=send, recv_sem=recv,
            device_id={"tp": device}, device_id_type=MESH,
        )

    def along_z(m, slot, source):
        return to(source, q_all.at[m, slot, y], qz_send.at[m, slot], qz_recv.at[m, slot], other_z[m])

    def along_y(m, slot, turn, source):
        return to(
            source, q_all.at[m, slot, y], qy_send.at[m, slot, turn], qy_recv.at[m, slot, y],
            z * ny + lax.rem(y + turn, ny),
        )

    def across_both(m, turn):
        return to(
            q_own.at[m], q_all.at[m, 0, y], qy_send.at[m, 0, turn], qy_recv.at[m, 0, y],
            sides[m] + lax.rem(y + turn, ny),
        )

    def from_y(m, slot, turn):
        there = lax.rem(y + turn, ny)
        return to(
            q_all.at[m, slot, there], q_all.at[m, slot, there],
            qy_send.at[m, slot, turn], qy_recv.at[m, slot, there], z * ny + there,
        )

    def ring(m, slot, h):
        at = pl.ds(h * half, half + h * EXTRA)
        return (
            to(sent_s.at[m, slot, h], got_s.at[m, slot + 1, h],
               r_send.at[m, slot, h, 0], r_recv.at[m, slot, h, 0], other_z[m]),
            to(sent_v.at[m, slot, at], got_v.at[m, slot + 1, at],
               r_send.at[m, slot, h, 1], r_recv.at[m, slot, h, 1], other_z[m]),
        )

    def final(m, there, i):
        at = pl.ds(pl.multiple_of(there * rows, 32), rows)
        low = pl.ds(deep, EXTRA)
        peer = z * ny + there
        src = (sent_v.at[m, nz - 1, at], sent_s.at[m, nz - 1], sent_v.at[m, nz - 1, low])[i]
        dst = (far_v, far_s, far_d)[i].at[m, y]
        return to(src, dst, f_send.at[m, there, i], f_recv.at[m, y, i], peer)

    def final_from(m, there):
        peer = z * ny + there
        return tuple(
            to(ref.at[m, there], ref.at[m, there], f_send.at[m, there, i], f_recv.at[m, there, i], peer)
            for i, ref in enumerate((far_v, far_s, far_d))
        )

    pl.semaphore_wait(barrier, 3 * ny - 1 + tp_count - 1)
    for m in range(2):
        along_z(m, 0, q_own.at[m]).start()
    for turn in (1, 3, 2):
        for m in range(2):
            across_both(m, turn).start()

    def columns_to(turn):
        there = lax.rem(mine + turn, tp_count)
        return across(
            w_out.at[:, pl.ds(pl.multiple_of(there * span, span), span)], cols.at[mine],
            c_send.at[turn], c_recv.at[turn], there,
        )

    def pass_on(slot):
        for m in range(2):
            along_z(m, slot, q_own.at[m]).wait_recv()

            @pl.when(slot < nz - 2)
            def _():
                along_z(m, slot + 1, q_all.at[m, slot, y]).start()

            @pl.when(slot > 0)
            def _():
                for turn in range(1, ny):
                    along_y(m, slot, turn, q_all.at[m, slot, y]).start()

    up = lax.broadcasted_iota(jnp.int32, (2 * TILE, 2 * TILE), 0)
    right = lax.broadcasted_iota(jnp.int32, (2 * TILE, 2 * TILE), 1)
    sort = jnp.where(right < TILE, 2 * right, 2 * right - 2 * TILE + 1) == up
    sort = sort.astype(jnp.float32).astype(jnp.bfloat16)

    def split(i, carry):
        block = pairs[pl.ds(pl.multiple_of(i * 2 * TILE, 2 * TILE), 2 * TILE), :]
        turned = lax.dot_general(
            block, sort, (((0,), (0,)), ((), ())), preferred_element_type=jnp.float32
        ).astype(jnp.bfloat16)
        at = pl.ds(pl.multiple_of(i * TILE, TILE), TILE)
        kt[0, :, at] = turned[:, :TILE]
        kt[1, :, at] = turned[:, TILE:]
        return carry

    wk_load.wait()
    made = jnp.dot(spaced[...], wk[...], preferred_element_type=jnp.float32).astype(jnp.bfloat16)
    for m in range(2):
        new_keys[m] = made[m * tall : (m + 1) * tall]
    pairs_load.wait()
    lax.fori_loop(0, cached // TILE // 2, split, 0)
    pass_on(0)
    wv_load.wait()
    new_values[...] = jnp.dot(normed[...], wv[...], preferred_element_type=jnp.float32).astype(jnp.bfloat16)
    lax.fori_loop(cached // TILE // 2, cached // TILE, split, 0)
    pass_on(1)
    for turn in range(1, tp_count):
        columns_to(turn).start()
    key_lane = lax.broadcasted_iota(jnp.int32, (1, cached), 1)
    bias[...] = jnp.where(me * cached + key_lane < prompt_len[...], 0.0, HIDDEN)
    values[cached : cached + rows] = new_values[:rows]
    values[cached + rows :] = jnp.zeros((total_keys - cached - rows, wide), jnp.bfloat16)
    for m in range(2):
        fresh = jnp.concatenate(
            [new_keys[m, :rows].astype(jnp.float32), jnp.zeros((TILE - rows, dims), jnp.float32)], axis=0
        )
        kt[m, :, cached:] = jnp.transpose(fresh).astype(jnp.bfloat16)
    up = lax.broadcasted_iota(jnp.int32, (2 * TILE, TILE), 0)
    right = lax.broadcasted_iota(jnp.int32, (2 * TILE, TILE), 1)
    halves[...] = (up // 2 == right).astype(jnp.float32).astype(jnp.bfloat16)
    for copy in last_loads:
        copy.wait()

    def score(m, h, slot, off):
        q = q_all[m, slot, 2 * h : 2 * h + 2, :rows].reshape(half, dims)
        buf = m
        best = None
        for c in range(0, cached, 256):
            s = jnp.dot(q, kt[m, :, c : c + 256], preferred_element_type=jnp.float32)
            s = s + bias[:, c : c + 256]
            scores[buf, :, c : c + 256] = s
            for j in range(0, 256, TILE):
                p = s[:, j : j + TILE]
                best = p if best is None else jnp.maximum(best, p)
        tail = jnp.dot(q, kt[m, :, cached:], preferred_element_type=jnp.float32)
        lane = lax.broadcasted_iota(jnp.int32, tail.shape, 1)
        row = lax.broadcasted_iota(jnp.int32, tail.shape, 0)
        gap = jnp.where(lane < rows, lane - row, 1 << 20)
        tail = jnp.where(gap <= off, tail, HIDDEN)
        scores[buf, :, cached:] = tail
        best = jnp.maximum(best, tail)
        return jnp.max(best, axis=1, keepdims=True)

    def weigh(m, h, top):
        buf = m
        part = None
        for c in range(0, total_keys, TILE):
            w = jnp.exp2((scores[buf, :, c : c + TILE] - top) * fold)
            weights[buf, :, c : c + TILE] = w.astype(jnp.bfloat16)
            part = w if part is None else part + w
        total = jnp.sum(part, axis=1, keepdims=True)
        return jnp.dot(weights[buf], values[...], preferred_element_type=jnp.float32), total

    def decode(m, slot, home):
        q = q_all[m, slot, 0, rows:].astype(jnp.float32)
        for there in range(1, ny):
            q = q + q_all[m, slot, there, rows:].astype(jnp.float32)
        qb = q.astype(jnp.bfloat16)
        row = lax.broadcasted_iota(jnp.int32, (EXTRA, 2 * slots), 0)
        lane = lax.broadcasted_iota(jnp.int32, (EXTRA, 2 * slots), 1)
        s = jnp.zeros((EXTRA, 2 * slots), jnp.float32)
        lens = jnp.zeros((EXTRA, 2 * slots), jnp.int32)
        for there in range(ny):
            seq = home * ny + there
            at = pl.ds(pl.multiple_of(seq * 2 * slots, 2 * slots), 2 * slots)
            one = lax.dot_general(
                qb, step_k[at, :], (((1,), (1,)), ((), ())), preferred_element_type=jnp.float32
            )
            s = jnp.where(row == there, one, s)
            lens = jnp.where(row == there, step_lens[seq], lens)
        seen = (lax.rem(lane, 2) == m) & (me * slots + lane // 2 < lens)
        s = jnp.where(seen, s, HIDDEN)
        own = jnp.sum(q * new_keys[m, rows:].astype(jnp.float32)[:1], axis=1, keepdims=True)
        mine = jnp.where(slot == nz - 1, y, EXTRA)
        own = jnp.where(row[:, :1] == mine, own, HIDDEN)
        top = jnp.maximum(jnp.max(s, axis=1, keepdims=True), own)
        w = jnp.exp2((s - top) * fold)
        own_w = jnp.exp2((own - top) * fold)
        total = jnp.sum(w, axis=1, keepdims=True) + own_w
        packed = jnp.dot(
            w.astype(jnp.bfloat16), halves[...], preferred_element_type=jnp.float32
        ).astype(jnp.bfloat16)
        wide_row = lax.broadcasted_iota(jnp.int32, (EXTRA, wide), 0)
        summed = jnp.zeros((EXTRA, wide), jnp.float32)
        for there in range(ny):
            seq = home * ny + there
            at = pl.ds(pl.multiple_of(seq * slots, slots), slots)
            one = jnp.dot(packed, step_v[at, :], preferred_element_type=jnp.float32)
            summed = jnp.where(wide_row == there, one, summed)
        own_w = own_w.astype(jnp.bfloat16).astype(jnp.float32)
        summed = summed + own_w * new_values[rows:].astype(jnp.float32)[:1]
        return top, total, summed

    def join(m, h, slot, top, total, summed):
        at = pl.ds(h * half, half + h * EXTRA)
        old = got_s[m, slot, h]
        places = [(2 * blocks * j, blocks) for j in range(2)] + [(4 * blocks, 2)] * h
        old_top = jnp.concatenate([spread(old, first, n, TILE) for first, n in places], axis=0)
        old_total = jnp.concatenate([spread(old, first + n, n, TILE) for first, n in places], axis=0)
        best = jnp.maximum(old_top, top)
        old_scale = jnp.exp2((old_top - best) * fold)
        new_scale = jnp.exp2((top - best) * fold)
        norm = old_total * old_scale + total * new_scale
        for c in range(0, wide, TILE):
            mixed = got_v[m, slot, at, c : c + TILE].astype(jnp.float32) * old_scale
            mixed = mixed + summed[:, c : c + TILE] * new_scale
            sent_v[m, slot, at, c : c + TILE] = mixed.astype(jnp.bfloat16)
        columns = []
        line = 0
        for first, n in places:
            for i in range(n):
                columns.append((first + i, best[line : line + 8]))
                columns.append((first + n + i, norm[line : line + 8]))
                line += 8
        sent_s[m, slot, h] = pack_columns(columns)

    units = [(m, h) for h in range(2) for m in range(2)]

    def turn_step(slot, carry):
        for m in range(2):
            for turn in range(1, ny):
                from_y(m, slot, turn).wait_recv()
        homes = [lax.rem(z + nz - 1 - slot, nz), lax.rem(z + 1 + slot, nz)]
        offs = [[(homes[m] * ny + 2 * h - me) * rows for h in range(2)] for m in range(2)]
        tops = [None] * len(units)
        tops[0] = score(0, 0, slot, offs[0][0])
        for u, (m, h) in enumerate(units):
            if u + 1 < len(units):
                m2, h2 = units[u + 1]
                tops[u + 1] = score(m2, h2, slot, offs[m2][h2])
            top = tops[u]
            summed, total = weigh(m, h, top)
            if h == 1:
                low = decode(m, slot, homes[m])
                top, total, summed = [
                    jnp.concatenate([p, q], axis=0) for p, q in zip((top, total, summed), low)
                ]

            @pl.when(slot > 0)
            def _():
                for copy in ring(m, slot - 1, h):
                    copy.wait_recv()

            join(m, h, slot, top, total, summed)

            @pl.when(slot < nz - 1)
            def _():
                for copy in ring(m, slot, h):
                    copy.start()

            if u == 1:
                @pl.when(slot < nz - 3)
                def _():
                    pass_on(slot + 2)

                @pl.when(slot == nz - 3)
                def _():
                    for m2 in range(2):
                        for turn in range(1, ny):
                            along_y(m2, nz - 1, turn, q_own.at[m2]).start()

            @pl.when(slot == nz - 1)
            def _():
                for there in range(ny):
                    @pl.when(y != there)
                    def _():
                        picks = [0] * (there // 2 == h) + [1, 2] * h
                        for i in picks:
                            final(m, there, i).start()
        return carry

    lax.fori_loop(0, nz, turn_step, 0)

    odd = lax.rem(y, 2) == 1

    def own_half(stats):
        return jnp.where(odd, pltpu.roll(stats, TILE - 2 * blocks, 1), stats)

    def merge(vals, tops, totals):
        best = functools.reduce(jnp.maximum, tops)
        scales = [jnp.exp2((t - best) * fold) for t in tops]
        norm = functools.reduce(jnp.add, [a * b for a, b in zip(scales, totals)])
        total = functools.reduce(jnp.add, [a * b.astype(jnp.float32) for a, b in zip(scales, vals)])
        return total / norm

    peers = [lax.rem(y + turn, ny) for turn in range(1, ny)]
    cut = 32
    gathered = []
    for m in range(2):
        for there in peers:
            for copy in final_from(m, there):
                copy.wait_recv()
        stats = [own_half(sent_s[m, nz - 1, y // 2])] + [own_half(far_s[m, there, y // 2]) for there in peers]
        parts = []
        for j in range(rows // cut):
            at = pl.ds(pl.multiple_of(y * rows + j * cut, cut), cut)
            vals = [sent_v[m, nz - 1, at, :]]
            vals += [far_v[m, there, j * cut : (j + 1) * cut, :] for there in peers]
            first = j * cut // 8
            parts.append(
                merge(
                    vals,
                    [spread(s, first, cut // 8, wide) for s in stats],
                    [spread(s, blocks + first, cut // 8, wide) for s in stats],
                )
            )
        stats = [sent_s[m, nz - 1, 1]] + [far_s[m, there, 1] for there in peers]
        parts.append(
            merge(
                [sent_v[m, nz - 1, deep:]] + [far_d[m, there] for there in peers],
                [spread(s, 4 * blocks, 2, wide) for s in stats],
                [spread(s, 4 * blocks + 2, 2, wide) for s in stats],
            )
        )
        gathered.append(parts)
    mixed = [mix_maps(one, two, ratio[...], gain[...]) for one, two in zip(*gathered)]
    for j in range(rows // cut):
        heads[mine, j * cut : (j + 1) * cut] = mixed[j]
    lines = mixed[-1].astype(jnp.float32)
    place = lax.broadcasted_iota(jnp.int32, lines.shape, 0)
    line = jnp.sum(jnp.where(place == y, lines, 0.0), axis=0, keepdims=True)
    heads[mine, rows:] = jnp.where(place == 0, line, 0.0).astype(jnp.bfloat16)

    def heads_to(turn):
        there = lax.rem(chip + turn, chips) * 2 + core
        return across(heads.at[mine], heads.at[mine], h_send.at[turn], h_recv.at[turn], there)

    def heads_over(turn):
        whose = lax.rem(chip + chips - turn, chips) * 2 + core
        return across(
            heads.at[whose], heads.at[whose], d_send.at[turn], d_recv.at[turn], chip * 2 + 1 - core
        )

    for turn in (2, 1, 3):
        heads_to(turn).start()
    heads_over(0).start()

    for m in range(2):
        for there in range(ny):
            @pl.when(y != there)
            def _():
                for i in range(3):
                    final(m, there, i).wait_send()
        for turn in range(1, ny):
            along_y(m, nz - 1, turn, q_own.at[m]).wait_send()

    def drain(slot, carry):
        for m in range(2):
            along_z(m, slot, q_own.at[m]).wait_send()
            for turn in range(1, ny):
                along_y(m, slot, turn, q_own.at[m]).wait_send()
            for h in range(2):
                for copy in ring(m, slot, h):
                    copy.wait_send()
        return carry

    lax.fori_loop(0, nz - 1, drain, 0)
    for turn in range(1, tp_count):
        columns_to(turn).wait()

    def term(whose):
        return jnp.dot(heads[whose], cols[whose], preferred_element_type=jnp.float32)

    total = term(mine)
    heads_over(0).wait_recv()
    total = total + term(chip * 2 + 1 - core)
    for turn in (1, 3, 2):
        heads_to(turn).wait_recv()
        heads_over(turn).start()
        total = total + term(lax.rem(chip + chips - turn, chips) * 2 + core)
    for turn in (1, 3, 2):
        heads_over(turn).wait_recv()
        total = total + term(lax.rem(chip + chips - turn, chips) * 2 + 1 - core)
    piece_out[...] = total[:rows].astype(jnp.bfloat16)
    step_out[...] = total[rows:][:1].astype(jnp.bfloat16)
    for turn in range(chips):
        if turn > 0:
            heads_to(turn).wait_send()
        heads_over(turn).wait_send()


def ring_attend(
    step_lens, ratio, prompt_len, gain, piece, step, scale_in, w_query, w_key, w_value,
    prompt_keys, prompt_values, cache_keys, cache_values, w_out, kv_count, tp_count, collective,
):
    rows, model = piece.shape
    tall = rows + EXTRA
    dims = w_query.shape[1]
    wide = w_value.shape[1]
    cached = prompt_values.shape[0]
    keys = cached + TILE
    ny = SIDE_Y
    nz = kv_count // ny
    deep = ny * rows + EXTRA
    span = w_out.shape[1] // tp_count
    smem = pl.BlockSpec(memory_space=pltpu.SMEM)
    vmem = pl.BlockSpec(memory_space=pltpu.VMEM)
    far = pl.BlockSpec(memory_space=pltpu.MemorySpace.HBM)
    dma = pltpu.SemaphoreType.DMA
    half = jnp.bfloat16
    fold = dims ** (-0.5) * math.log2(math.e)
    return pl.pallas_call(
        functools.partial(ring_kernel, kv_count, tp_count, fold),
        out_shape=[
            jax.ShapeDtypeStruct((rows, span), half),
            jax.ShapeDtypeStruct((1, span), half),
            jax.ShapeDtypeStruct((2, tall, dims), half),
            jax.ShapeDtypeStruct((tall, wide), half),
        ],
        in_specs=[smem] + [vmem] * 3 + [far] * 11,
        out_specs=[vmem] * 4,
        scratch_shapes=[
            pltpu.VMEM((tall, model), half),
            pltpu.VMEM(step.shape, half),
            pltpu.VMEM(scale_in.shape, jnp.float32),
            pltpu.VMEM(w_query.shape, half),
            pltpu.VMEM(w_key.shape, half),
            pltpu.VMEM(w_value.shape, half),
            pltpu.VMEM((tall, model), half),
            pltpu.VMEM((2 * tall, 2 * model), half),
            pltpu.VMEM((2 * tall, dims), half),
            pltpu.VMEM((2, tall, dims), half),
            pltpu.VMEM((2, nz, ny, tall, dims), half),
            pltpu.VMEM(prompt_keys.shape, half),
            pltpu.VMEM((2, dims, keys), half),
            pltpu.VMEM((keys, wide), half),
            pltpu.VMEM((1, cached), jnp.float32),
            pltpu.VMEM((2 * TILE, TILE), half),
            pltpu.VMEM(cache_keys.shape, half),
            pltpu.VMEM(cache_values.shape, half),
            pltpu.VMEM((2, 2 * rows, keys), jnp.float32),
            pltpu.VMEM((2, 2 * rows, keys), half),
            pltpu.VMEM((2, nz, deep, wide), half),
            pltpu.VMEM((2, nz, 2, 8, TILE), jnp.float32),
            pltpu.VMEM((2, nz, deep, wide), half),
            pltpu.VMEM((2, nz, 2, 8, TILE), jnp.float32),
            pltpu.VMEM((2, ny, rows, wide), half),
            pltpu.VMEM((2, ny, 2, 8, TILE), jnp.float32),
            pltpu.VMEM((2, ny, EXTRA, wide), half),
            pltpu.VMEM((tp_count, wide, span), half),
            pltpu.VMEM((tp_count, tall, wide), half),
            dma((11,)),
            dma((2, nz)), dma((2, nz)),
            dma((2, nz, ny)), dma((2, nz, ny)),
            dma((2, nz, 2, 2)), dma((2, nz, 2, 2)),
            dma((2, ny, 3)), dma((2, ny, 3)),
            dma((tp_count,)), dma((tp_count,)),
            dma((tp_count // 2,)), dma((tp_count // 2,)),
            dma((tp_count // 2,)), dma((tp_count // 2,)),
        ],
        compiler_params=pltpu.CompilerParams(
            collective_id=collective, has_side_effects=True, vmem_limit_bytes=62 * 1024 * 1024
        ),
        name="ring_attend",
    )(
        step_lens, ratio, prompt_len, gain, piece, step, scale_in, w_query, w_key, w_value,
        prompt_keys, prompt_values, cache_keys, cache_values, w_out,
    )


def on_device(
    kv_count,
    tp_count,
    piece_tokens,
    step_tokens,
    in_gain,
    w_query,
    w_key,
    w_value,
    w_out,
    mix_ratio,
    out_gain,
    prompt_keys,
    prompt_values,
    step_cache_keys,
    step_cache_values,
    prompt_len,
    step_lens,
):
    piece_dev = piece_tokens.shape[0]
    step_dev = step_tokens.shape[0]
    heads, maps, dims = w_query.shape[1:]
    wide = w_value.shape[-1]
    mixed, line, key_rows, value_rows = ring_attend(
        step_lens,
        mix_ratio[None, :],
        prompt_len[None, :],
        out_gain[None, :],
        piece_tokens,
        step_tokens,
        in_gain[None, :],
        w_query.reshape(-1, dims),
        w_key.reshape(-1, dims),
        w_value.reshape(-1, wide),
        prompt_keys.reshape(-1, dims),
        prompt_values.reshape(-1, wide),
        step_cache_keys.reshape(-1, dims),
        step_cache_values.reshape(-1, wide),
        w_out.reshape(-1, w_out.shape[-1]),
        kv_count,
        tp_count,
        0,
    )
    piece_out, step_out, piece_k, piece_v, step_k, step_v = finish(mixed, line, key_rows, value_rows)
    return (
        piece_out,
        step_out,
        piece_k.reshape(piece_dev, heads, maps, dims),
        piece_v.reshape(piece_dev, heads, wide),
        step_k.reshape(step_dev, heads, maps, dims),
        step_v.reshape(step_dev, heads, wide),
    )


def solution(mesh):
    in_specs = (
        P("kv", None),
        P("kv", None),
        P(),
        P(None, "tp", None, None),
        P(None, "tp", None, None),
        P(None, "tp", None),
        P("tp", None, None),
        P("tp"),
        P(),
        P("kv", "tp", None, None),
        P("kv", "tp", None),
        P(None, "kv", "tp", None, None),
        P(None, "kv", "tp", None),
        P(),
        P(),
    )
    out_specs = (
        P("kv", "tp"),
        P("kv", "tp"),
        P("kv", "tp", None, None),
        P("kv", "tp", None),
        P("kv", "tp", None, None),
        P("kv", "tp", None),
    )
    return jax.shard_map(
        functools.partial(on_device, mesh.shape["kv"], mesh.shape["tp"]),
        mesh=mesh, in_specs=in_specs, out_specs=out_specs, check_vma=False
    )
```

```python
import functools
import math

import jax
import jax.numpy as jnp
from jax import lax
from jax.experimental import pallas as pl
from jax.experimental.pallas import tpu as pltpu
from jax.sharding import PartitionSpec as P

EPS = 1e-06
OUT_SCALE = 0.8
MESH = pl.DeviceIdType.MESH
HIDDEN = -1e30


def finish_kernel(mixed, line, keys, vals, piece_out, step_out, piece_k, piece_v, step_k, step_v):
    rows = piece_out.shape[0]
    piece_out[...] = mixed[...]
    step_out[...] = line[...]
    piece_v[...] = vals[:rows]
    step_v[...] = vals[rows:].astype(jnp.float32)[:1].astype(jnp.bfloat16)
    up = lax.broadcasted_iota(jnp.int32, (2 * rows, rows), 0)
    right = lax.broadcasted_iota(jnp.int32, (2 * rows, rows), 1)
    total = None
    for m in range(2):
        pick = (up == 2 * right + m).astype(jnp.float32).astype(jnp.bfloat16)
        part = jnp.dot(pick, keys[m, :rows], preferred_element_type=jnp.float32)
        total = part if total is None else total + part
    piece_k[...] = total.astype(jnp.bfloat16)
    both = [keys[m, rows:].astype(jnp.float32)[:1] for m in range(2)]
    step_k[...] = jnp.concatenate(both, axis=0).astype(jnp.bfloat16)


def finish(mixed, line, keys, vals):
    rows, span = mixed.shape
    dims = keys.shape[-1]
    wide = vals.shape[-1]
    vmem = pl.BlockSpec(memory_space=pltpu.VMEM)
    shapes = [(rows, span), (1, span), (2 * rows, dims), (rows, wide), (2, dims), (1, wide)]
    return pl.pallas_call(
        finish_kernel,
        out_shape=[jax.ShapeDtypeStruct(shape, jnp.bfloat16) for shape in shapes],
        in_specs=[vmem] * 4,
        out_specs=[vmem] * 6,
        compiler_params=pltpu.CompilerParams(vmem_limit_bytes=62 * 1024 * 1024),
        name="finish",
    )(mixed, line, keys, vals)


def mix_maps(first, second, ratio, gain):
    mixed = first - ratio * second
    inv_rms = lax.rsqrt(jnp.mean(mixed * mixed, axis=-1, keepdims=True) + EPS)
    return (mixed * inv_rms * gain * OUT_SCALE).astype(jnp.bfloat16)


SIDE_Y = 4
TILE = 128
EXTRA = 8


def spread(stats, first, groups, width):
    cols = [jnp.broadcast_to(stats[:, i : i + 1], (8, width)) for i in range(first, first + groups)]
    return jnp.concatenate(cols, axis=0)


def pack_columns(columns):
    lane = lax.broadcasted_iota(jnp.int32, (8, TILE), 1)
    out = jnp.zeros((8, TILE), jnp.float32)
    for place, column in columns:
        out = jnp.where(lane == place, column, out)
    return out


def ring_kernel(
    kv_count, tp_count, fold, step_lens, ratio, prompt_len, gain,
    piece, step, scale_in, w_query, w_key, w_value,
    prompt_keys, prompt_values, cache_keys, cache_values, w_out, piece_out, step_out, new_keys, new_values,
    tokens, step_token, scales, wq, wk, wv, normed, spaced, both, q_own, q_all, pairs, kt, values, bias, halves, step_k, step_v, scores, weights,
    sent_v, sent_s, got_v, got_s, far_v, far_s, far_d, cols, heads,
    load_sem, qz_send, qz_recv, qy_send, qy_recv, r_send, r_recv, f_send, f_recv,
    c_send, c_recv, h_send, h_recv, d_send, d_recv,
):
    ny = SIDE_Y
    nz = kv_count // ny
    tall, dims = new_keys.shape[1:]
    model = piece.shape[1]
    rows = tall - EXTRA
    wide = values.shape[1]
    cached = bias.shape[1]
    total_keys = values.shape[0]
    slots = step_v.shape[0] // kv_count
    half = 2 * rows
    blocks = rows // 8
    deep = 2 * half
    me = lax.axis_index("kv")
    z = me // ny
    y = lax.rem(me, ny)
    other_z = [lax.rem(z + 1, nz) * ny + y, lax.rem(z + nz - 1, nz) * ny + y]
    mine = lax.axis_index("tp")
    chips = tp_count // 2
    chip = mine // 2
    core = lax.rem(mine, 2)
    span = piece_out.shape[1]

    def load(i, source, target):
        copy = pltpu.make_async_copy(source, target, load_sem.at[i])
        copy.start()
        return copy

    first_loads = [
        load(0, piece, tokens.at[pl.ds(0, rows)]),
        load(1, step, step_token),
        load(2, scale_in, scales),
    ]
    wq_load = load(3, w_query, wq)
    wk_load = load(4, w_key, wk)
    pairs_load = load(5, prompt_keys, pairs)
    wv_load = load(6, w_value, wv)
    last_loads = [
        load(7, prompt_values, values.at[pl.ds(0, cached)]),
        load(8, cache_keys, step_k),
        load(9, cache_values, step_v),
        load(10, w_out.at[:, pl.ds(pl.multiple_of(mine * span, span), span)], cols.at[mine]),
    ]

    barrier = pltpu.get_barrier_semaphore()
    sides = [lax.rem(z + 1, nz) * ny, lax.rem(z + nz - 1, nz) * ny]
    for side in sides + [z * ny]:
        for turn in range(side is not sides[0] and side is not sides[1], ny):
            there = side + lax.rem(y + turn, ny)
            pl.semaphore_signal(barrier, inc=1, device_id={"kv": there}, device_id_type=MESH)
    for turn in range(1, tp_count):
        there = lax.rem(mine + turn, tp_count)
        pl.semaphore_signal(barrier, inc=1, device_id={"tp": there}, device_id_type=MESH)

    for m in range(2):
        got_v[m, 0] = jnp.zeros(got_v.shape[2:], jnp.bfloat16)
        lane = lax.broadcasted_iota(jnp.int32, (8, TILE), 1)
        spot = jnp.where(lane < 4 * blocks, lax.rem(lane, 2 * blocks), lane - 4 * blocks + blocks - EXTRA // 8)
        for h in range(2):
            got_s[m, 0, h] = jnp.where(spot < blocks, HIDDEN, 0.0)
    up = lax.broadcasted_iota(jnp.int32, (TILE, 4 * TILE), 0)
    right = lax.broadcasted_iota(jnp.int32, (TILE, 4 * TILE), 1)
    gap = jnp.where(right < 2 * TILE, 2 * up, 2 * up + 2 * TILE + 1)
    open_up = (gap == right).astype(jnp.float32).astype(jnp.bfloat16)

    for copy in first_loads:
        copy.wait()
    place = lax.broadcasted_iota(jnp.int32, (EXTRA, model), 0)
    low = jnp.broadcast_to(step_token[...].astype(jnp.float32), (EXTRA, model))
    tokens[rows:] = jnp.where(place == 0, low, 0.0).astype(jnp.bfloat16)

    def norm(i, carry):
        at = pl.ds(pl.multiple_of(i * EXTRA, EXTRA), EXTRA)
        floats = tokens[at, :].astype(jnp.float32)
        inv_rms = lax.rsqrt(jnp.mean(floats * floats, axis=-1, keepdims=True) + EPS)
        normed[at, :] = (floats * inv_rms * scales[...]).astype(jnp.bfloat16)
        return carry

    lax.fori_loop(0, tall // EXTRA, norm, 0)
    for i in range(model // TILE):
        wider = jnp.dot(normed[:, i * TILE : (i + 1) * TILE], open_up, preferred_element_type=jnp.float32)
        for m in range(2):
            slab = wider[:, m * 2 * TILE : (m + 1) * 2 * TILE]
            spaced[m * tall : (m + 1) * tall, i * 2 * TILE : (i + 1) * 2 * TILE] = slab.astype(jnp.bfloat16)
    wq_load.wait()
    both[...] = jnp.dot(spaced[...], wq[...], preferred_element_type=jnp.float32).astype(jnp.bfloat16)
    extra_row = lax.broadcasted_iota(jnp.int32, (EXTRA, dims), 0)
    for m in range(2):
        q_own[m, :rows] = both[m * tall : m * tall + rows]
        line = both[m * tall + rows : (m + 1) * tall].astype(jnp.float32)[:1]
        q_own[m, rows:] = jnp.where(extra_row == y, line, 0.0).astype(jnp.bfloat16)
        q_all[m, nz - 1, y] = q_own[m]

    def to(src, dst, send, recv, device):
        return pltpu.make_async_remote_copy(
            src_ref=src, dst_ref=dst, send_sem=send, recv_sem=recv,
            device_id={"kv": device}, device_id_type=MESH,
        )

    def across(src, dst, send, recv, device):
        return pltpu.make_async_remote_copy(
            src_ref=src, dst_ref=dst, send_sem=send, recv_sem=recv,
            device_id={"tp": device}, device_id_type=MESH,
        )

    def along_z(m, slot, source):
        return to(source, q_all.at[m, slot, y], qz_send.at[m, slot], qz_recv.at[m, slot], other_z[m])

    def along_y(m, slot, turn, source):
        return to(
            source, q_all.at[m, slot, y], qy_send.at[m, slot, turn], qy_recv.at[m, slot, y],
            z * ny + lax.rem(y + turn, ny),
        )

    def across_both(m, turn):
        return to(
            q_own.at[m], q_all.at[m, 0, y], qy_send.at[m, 0, turn], qy_recv.at[m, 0, y],
            sides[m] + lax.rem(y + turn, ny),
        )

    def from_y(m, slot, turn):
        there = lax.rem(y + turn, ny)
        return to(
            q_all.at[m, slot, there], q_all.at[m, slot, there],
            qy_send.at[m, slot, turn], qy_recv.at[m, slot, there], z * ny + there,
        )

    def ring(m, slot, h):
        at = pl.ds(h * half, half + h * EXTRA)
        return (
            to(sent_s.at[m, slot, h], got_s.at[m, slot + 1, h],
               r_send.at[m, slot, h, 0], r_recv.at[m, slot, h, 0], other_z[m]),
            to(sent_v.at[m, slot, at], got_v.at[m, slot + 1, at],
               r_send.at[m, slot, h, 1], r_recv.at[m, slot, h, 1], other_z[m]),
        )

    def final(m, there, i):
        at = pl.ds(pl.multiple_of(there * rows, 32), rows)
        low = pl.ds(deep, EXTRA)
        peer = z * ny + there
        src = (sent_v.at[m, nz - 1, at], sent_s.at[m, nz - 1], sent_v.at[m, nz - 1, low])[i]
        dst = (far_v, far_s, far_d)[i].at[m, y]
        return to(src, dst, f_send.at[m, there, i], f_recv.at[m, y, i], peer)

    def final_from(m, there):
        peer = z * ny + there
        return tuple(
            to(ref.at[m, there], ref.at[m, there], f_send.at[m, there, i], f_recv.at[m, there, i], peer)
            for i, ref in enumerate((far_v, far_s, far_d))
        )

    pl.semaphore_wait(barrier, 3 * ny - 1 + tp_count - 1)
    for m in range(2):
        along_z(m, 0, q_own.at[m]).start()
    for turn in (1, 3, 2):
        for m in range(2):
            across_both(m, turn).start()

    def columns_to(turn):
        there = lax.rem(mine + turn, tp_count)
        return across(
            w_out.at[:, pl.ds(pl.multiple_of(there * span, span), span)], cols.at[mine],
            c_send.at[turn], c_recv.at[turn], there,
        )

    def pass_on(slot):
        for m in range(2):
            along_z(m, slot, q_own.at[m]).wait_recv()

            @pl.when(slot < nz - 2)
            def _():
                along_z(m, slot + 1, q_all.at[m, slot, y]).start()

            @pl.when(slot > 0)
            def _():
                for turn in range(1, ny):
                    along_y(m, slot, turn, q_all.at[m, slot, y]).start()

    up = lax.broadcasted_iota(jnp.int32, (2 * TILE, 2 * TILE), 0)
    right = lax.broadcasted_iota(jnp.int32, (2 * TILE, 2 * TILE), 1)
    sort = jnp.where(right < TILE, 2 * right, 2 * right - 2 * TILE + 1) == up
    sort = sort.astype(jnp.float32).astype(jnp.bfloat16)

    def split(i, carry):
        block = pairs[pl.ds(pl.multiple_of(i * 2 * TILE, 2 * TILE), 2 * TILE), :]
        turned = lax.dot_general(
            block, sort, (((0,), (0,)), ((), ())), preferred_element_type=jnp.float32
        ).astype(jnp.bfloat16)
        at = pl.ds(pl.multiple_of(i * TILE, TILE), TILE)
        kt[0, :, at] = turned[:, :TILE]
        kt[1, :, at] = turned[:, TILE:]
        return carry

    wk_load.wait()
    made = jnp.dot(spaced[...], wk[...], preferred_element_type=jnp.float32).astype(jnp.bfloat16)
    for m in range(2):
        new_keys[m] = made[m * tall : (m + 1) * tall]
    pairs_load.wait()
    lax.fori_loop(0, cached // TILE // 2, split, 0)
    pass_on(0)
    wv_load.wait()
    new_values[...] = jnp.dot(normed[...], wv[...], preferred_element_type=jnp.float32).astype(jnp.bfloat16)
    lax.fori_loop(cached // TILE // 2, cached // TILE, split, 0)
    pass_on(1)
    for turn in range(1, tp_count):
        columns_to(turn).start()
    key_lane = lax.broadcasted_iota(jnp.int32, (1, cached), 1)
    bias[...] = jnp.where(me * cached + key_lane < prompt_len[...], 0.0, HIDDEN)
    values[cached : cached + rows] = new_values[:rows]
    values[cached + rows :] = jnp.zeros((total_keys - cached - rows, wide), jnp.bfloat16)
    for m in range(2):
        fresh = jnp.concatenate(
            [new_keys[m, :rows].astype(jnp.float32), jnp.zeros((TILE - rows, dims), jnp.float32)], axis=0
        )
        kt[m, :, cached:] = jnp.transpose(fresh).astype(jnp.bfloat16)
    up = lax.broadcasted_iota(jnp.int32, (2 * TILE, TILE), 0)
    right = lax.broadcasted_iota(jnp.int32, (2 * TILE, TILE), 1)
    halves[...] = (up // 2 == right).astype(jnp.float32).astype(jnp.bfloat16)
    for copy in last_loads:
        copy.wait()

    def score(m, h, slot, off):
        q = q_all[m, slot, 2 * h : 2 * h + 2, :rows].reshape(half, dims)
        buf = m
        best = None
        for c in range(0, cached, 256):
            s = jnp.dot(q, kt[m, :, c : c + 256], preferred_element_type=jnp.float32)
            s = s + bias[:, c : c + 256]
            scores[buf, :, c : c + 256] = s
            for j in range(0, 256, TILE):
                p = s[:, j : j + TILE]
                best = p if best is None else jnp.maximum(best, p)
        tail = jnp.dot(q, kt[m, :, cached:], preferred_element_type=jnp.float32)
        lane = lax.broadcasted_iota(jnp.int32, tail.shape, 1)
        row = lax.broadcasted_iota(jnp.int32, tail.shape, 0)
        gap = jnp.where(lane < rows, lane - row, 1 << 20)
        tail = jnp.where(gap <= off, tail, HIDDEN)
        scores[buf, :, cached:] = tail
        best = jnp.maximum(best, tail)
        return jnp.max(best, axis=1, keepdims=True)

    def weigh(m, h, top):
        buf = m
        part = None
        for c in range(0, total_keys, TILE):
            w = jnp.exp2((scores[buf, :, c : c + TILE] - top) * fold)
            weights[buf, :, c : c + TILE] = w.astype(jnp.bfloat16)
            part = w if part is None else part + w
        total = jnp.sum(part, axis=1, keepdims=True)
        return jnp.dot(weights[buf], values[...], preferred_element_type=jnp.float32), total

    def decode(m, slot, home):
        q = q_all[m, slot, 0, rows:].astype(jnp.float32)
        for there in range(1, ny):
            q = q + q_all[m, slot, there, rows:].astype(jnp.float32)
        qb = q.astype(jnp.bfloat16)
        row = lax.broadcasted_iota(jnp.int32, (EXTRA, 2 * slots), 0)
        lane = lax.broadcasted_iota(jnp.int32, (EXTRA, 2 * slots), 1)
        s = jnp.zeros((EXTRA, 2 * slots), jnp.float32)
        lens = jnp.zeros((EXTRA, 2 * slots), jnp.int32)
        for there in range(ny):
            seq = home * ny + there
            at = pl.ds(pl.multiple_of(seq * 2 * slots, 2 * slots), 2 * slots)
            one = lax.dot_general(
                qb, step_k[at, :], (((1,), (1,)), ((), ())), preferred_element_type=jnp.float32
            )
            s = jnp.where(row == there, one, s)
            lens = jnp.where(row == there, step_lens[seq], lens)
        seen = (lax.rem(lane, 2) == m) & (me * slots + lane // 2 < lens)
        s = jnp.where(seen, s, HIDDEN)
        own = jnp.sum(q * new_keys[m, rows:].astype(jnp.float32)[:1], axis=1, keepdims=True)
        mine = jnp.where(slot == nz - 1, y, EXTRA)
        own = jnp.where(row[:, :1] == mine, own, HIDDEN)
        top = jnp.maximum(jnp.max(s, axis=1, keepdims=True), own)
        w = jnp.exp2((s - top) * fold)
        own_w = jnp.exp2((own - top) * fold)
        total = jnp.sum(w, axis=1, keepdims=True) + own_w
        packed = jnp.dot(
            w.astype(jnp.bfloat16), halves[...], preferred_element_type=jnp.float32
        ).astype(jnp.bfloat16)
        wide_row = lax.broadcasted_iota(jnp.int32, (EXTRA, wide), 0)
        summed = jnp.zeros((EXTRA, wide), jnp.float32)
        for there in range(ny):
            seq = home * ny + there
            at = pl.ds(pl.multiple_of(seq * slots, slots), slots)
            one = jnp.dot(packed, step_v[at, :], preferred_element_type=jnp.float32)
            summed = jnp.where(wide_row == there, one, summed)
        own_w = own_w.astype(jnp.bfloat16).astype(jnp.float32)
        summed = summed + own_w * new_values[rows:].astype(jnp.float32)[:1]
        return top, total, summed

    def join(m, h, slot, top, total, summed):
        at = pl.ds(h * half, half + h * EXTRA)
        old = got_s[m, slot, h]
        places = [(2 * blocks * j, blocks) for j in range(2)] + [(4 * blocks, EXTRA // 8)] * h
        old_top = jnp.concatenate([spread(old, first, n, TILE) for first, n in places], axis=0)
        old_total = jnp.concatenate([spread(old, first + n, n, TILE) for first, n in places], axis=0)
        best = jnp.maximum(old_top, top)
        old_scale = jnp.exp2((old_top - best) * fold)
        new_scale = jnp.exp2((top - best) * fold)
        norm = old_total * old_scale + total * new_scale
        for c in range(0, wide, TILE):
            mixed = got_v[m, slot, at, c : c + TILE].astype(jnp.float32) * old_scale
            mixed = mixed + summed[:, c : c + TILE] * new_scale
            sent_v[m, slot, at, c : c + TILE] = mixed.astype(jnp.bfloat16)
        columns = []
        line = 0
        for first, n in places:
            for i in range(n):
                columns.append((first + i, best[line : line + 8]))
                columns.append((first + n + i, norm[line : line + 8]))
                line += 8
        sent_s[m, slot, h] = pack_columns(columns)

    units = [(m, h) for h in range(2) for m in range(2)]

    def turn_step(slot, carry):
        for m in range(2):
            for turn in range(1, ny):
                from_y(m, slot, turn).wait_recv()
        homes = [lax.rem(z + nz - 1 - slot, nz), lax.rem(z + 1 + slot, nz)]
        offs = [[(homes[m] * ny + 2 * h - me) * rows for h in range(2)] for m in range(2)]
        tops = [None] * len(units)
        tops[0] = score(0, 0, slot, offs[0][0])
        for u, (m, h) in enumerate(units):
            if u + 1 < len(units):
                m2, h2 = units[u + 1]
                tops[u + 1] = score(m2, h2, slot, offs[m2][h2])
            top = tops[u]
            summed, total = weigh(m, h, top)
            if h == 1:
                low = decode(m, slot, homes[m])
                top, total, summed = [
                    jnp.concatenate([p, q], axis=0) for p, q in zip((top, total, summed), low)
                ]

            @pl.when(slot > 0)
            def _():
                for copy in ring(m, slot - 1, h):
                    copy.wait_recv()

            join(m, h, slot, top, total, summed)

            @pl.when(slot < nz - 1)
            def _():
                for copy in ring(m, slot, h):
                    copy.start()

            if u == 1:
                @pl.when(slot < nz - 3)
                def _():
                    pass_on(slot + 2)

                @pl.when(slot == nz - 3)
                def _():
                    for m2 in range(2):
                        for turn in range(1, ny):
                            along_y(m2, nz - 1, turn, q_own.at[m2]).start()

            @pl.when(slot == nz - 1)
            def _():
                for there in range(ny):
                    @pl.when(y != there)
                    def _():
                        picks = [0] * (there // 2 == h) + [1, 2] * h
                        for i in picks:
                            final(m, there, i).start()
        return carry

    lax.fori_loop(0, nz, turn_step, 0)

    odd = lax.rem(y, 2) == 1

    def own_half(stats):
        return jnp.where(odd, pltpu.roll(stats, TILE - 2 * blocks, 1), stats)

    def merge(vals, tops, totals):
        best = functools.reduce(jnp.maximum, tops)
        scales = [jnp.exp2((t - best) * fold) for t in tops]
        norm = functools.reduce(jnp.add, [a * b for a, b in zip(scales, totals)])
        total = functools.reduce(jnp.add, [a * b.astype(jnp.float32) for a, b in zip(scales, vals)])
        return total / norm

    peers = [lax.rem(y + turn, ny) for turn in range(1, ny)]
    cut = 32
    gathered = []
    for m in range(2):
        for there in peers:
            for copy in final_from(m, there):
                copy.wait_recv()
        stats = [own_half(sent_s[m, nz - 1, y // 2])] + [own_half(far_s[m, there, y // 2]) for there in peers]
        parts = []
        for j in range(rows // cut):
            at = pl.ds(pl.multiple_of(y * rows + j * cut, cut), cut)
            vals = [sent_v[m, nz - 1, at, :]]
            vals += [far_v[m, there, j * cut : (j + 1) * cut, :] for there in peers]
            first = j * cut // 8
            parts.append(
                merge(
                    vals,
                    [spread(s, first, cut // 8, wide) for s in stats],
                    [spread(s, blocks + first, cut // 8, wide) for s in stats],
                )
            )
        stats = [sent_s[m, nz - 1, 1]] + [far_s[m, there, 1] for there in peers]
        parts.append(
            merge(
                [sent_v[m, nz - 1, deep:]] + [far_d[m, there] for there in peers],
                [spread(s, 4 * blocks, EXTRA // 8, wide) for s in stats],
                [spread(s, 4 * blocks + EXTRA // 8, EXTRA // 8, wide) for s in stats],
            )
        )
        gathered.append(parts)
    mixed = [mix_maps(one, two, ratio[...], gain[...]) for one, two in zip(*gathered)]
    for j in range(rows // cut):
        heads[mine, j * cut : (j + 1) * cut] = mixed[j]
    lines = mixed[-1].astype(jnp.float32)
    place = lax.broadcasted_iota(jnp.int32, lines.shape, 0)
    line = jnp.sum(jnp.where(place == y, lines, 0.0), axis=0, keepdims=True)
    heads[mine, rows:] = jnp.where(place == 0, line, 0.0).astype(jnp.bfloat16)

    def heads_to(turn):
        there = lax.rem(chip + turn, chips) * 2 + core
        return across(heads.at[mine], heads.at[mine], h_send.at[turn], h_recv.at[turn], there)

    def heads_over(turn):
        whose = lax.rem(chip + chips - turn, chips) * 2 + core
        return across(
            heads.at[whose], heads.at[whose], d_send.at[turn], d_recv.at[turn], chip * 2 + 1 - core
        )

    for turn in (2, 1, 3):
        heads_to(turn).start()
    heads_over(0).start()

    for m in range(2):
        for there in range(ny):
            @pl.when(y != there)
            def _():
                for i in range(3):
                    final(m, there, i).wait_send()
        for turn in range(1, ny):
            along_y(m, nz - 1, turn, q_own.at[m]).wait_send()

    def drain(slot, carry):
        for m in range(2):
            along_z(m, slot, q_own.at[m]).wait_send()
            for turn in range(1, ny):
                along_y(m, slot, turn, q_own.at[m]).wait_send()
            for h in range(2):
                for copy in ring(m, slot, h):
                    copy.wait_send()
        return carry

    lax.fori_loop(0, nz - 1, drain, 0)
    for turn in range(1, tp_count):
        columns_to(turn).wait()

    def term(whose):
        return jnp.dot(heads[whose], cols[whose], preferred_element_type=jnp.float32)

    total = term(mine)
    heads_over(0).wait_recv()
    total = total + term(chip * 2 + 1 - core)
    for turn in (1, 3, 2):
        heads_to(turn).wait_recv()
        heads_over(turn).start()
        total = total + term(lax.rem(chip + chips - turn, chips) * 2 + core)
    for turn in (1, 3, 2):
        heads_over(turn).wait_recv()
        total = total + term(lax.rem(chip + chips - turn, chips) * 2 + 1 - core)
    piece_out[...] = total[:rows].astype(jnp.bfloat16)
    step_out[...] = total[rows:][:1].astype(jnp.bfloat16)
    for turn in range(chips):
        if turn > 0:
            heads_to(turn).wait_send()
        heads_over(turn).wait_send()


def ring_attend(
    step_lens, ratio, prompt_len, gain, piece, step, scale_in, w_query, w_key, w_value,
    prompt_keys, prompt_values, cache_keys, cache_values, w_out, kv_count, tp_count, collective,
):
    rows, model = piece.shape
    tall = rows + EXTRA
    dims = w_query.shape[1]
    wide = w_value.shape[1]
    cached = prompt_values.shape[0]
    keys = cached + TILE
    ny = SIDE_Y
    nz = kv_count // ny
    deep = ny * rows + EXTRA
    span = w_out.shape[1] // tp_count
    smem = pl.BlockSpec(memory_space=pltpu.SMEM)
    vmem = pl.BlockSpec(memory_space=pltpu.VMEM)
    far = pl.BlockSpec(memory_space=pltpu.MemorySpace.HBM)
    dma = pltpu.SemaphoreType.DMA
    half = jnp.bfloat16
    fold = dims ** (-0.5) * math.log2(math.e)
    return pl.pallas_call(
        functools.partial(ring_kernel, kv_count, tp_count, fold),
        out_shape=[
            jax.ShapeDtypeStruct((rows, span), half),
            jax.ShapeDtypeStruct((1, span), half),
            jax.ShapeDtypeStruct((2, tall, dims), half),
            jax.ShapeDtypeStruct((tall, wide), half),
        ],
        in_specs=[smem] + [vmem] * 3 + [far] * 11,
        out_specs=[vmem] * 4,
        scratch_shapes=[
            pltpu.VMEM((tall, model), half),
            pltpu.VMEM(step.shape, half),
            pltpu.VMEM(scale_in.shape, jnp.float32),
            pltpu.VMEM(w_query.shape, half),
            pltpu.VMEM(w_key.shape, half),
            pltpu.VMEM(w_value.shape, half),
            pltpu.VMEM((tall, model), half),
            pltpu.VMEM((2 * tall, 2 * model), half),
            pltpu.VMEM((2 * tall, dims), half),
            pltpu.VMEM((2, tall, dims), half),
            pltpu.VMEM((2, nz, ny, tall, dims), half),
            pltpu.VMEM(prompt_keys.shape, half),
            pltpu.VMEM((2, dims, keys), half),
            pltpu.VMEM((keys, wide), half),
            pltpu.VMEM((1, cached), jnp.float32),
            pltpu.VMEM((2 * TILE, TILE), half),
            pltpu.VMEM(cache_keys.shape, half),
            pltpu.VMEM(cache_values.shape, half),
            pltpu.VMEM((2, 2 * rows, keys), jnp.float32),
            pltpu.VMEM((2, 2 * rows, keys), half),
            pltpu.VMEM((2, nz, deep, wide), half),
            pltpu.VMEM((2, nz, 2, 8, TILE), jnp.float32),
            pltpu.VMEM((2, nz, deep, wide), half),
            pltpu.VMEM((2, nz, 2, 8, TILE), jnp.float32),
            pltpu.VMEM((2, ny, rows, wide), half),
            pltpu.VMEM((2, ny, 2, 8, TILE), jnp.float32),
            pltpu.VMEM((2, ny, EXTRA, wide), half),
            pltpu.VMEM((tp_count, wide, span), half),
            pltpu.VMEM((tp_count, tall, wide), half),
            dma((11,)),
            dma((2, nz)), dma((2, nz)),
            dma((2, nz, ny)), dma((2, nz, ny)),
            dma((2, nz, 2, 2)), dma((2, nz, 2, 2)),
            dma((2, ny, 3)), dma((2, ny, 3)),
            dma((tp_count,)), dma((tp_count,)),
            dma((tp_count // 2,)), dma((tp_count // 2,)),
            dma((tp_count // 2,)), dma((tp_count // 2,)),
        ],
        compiler_params=pltpu.CompilerParams(
            collective_id=collective, has_side_effects=True, vmem_limit_bytes=62 * 1024 * 1024
        ),
        name="ring_attend",
    )(
        step_lens, ratio, prompt_len, gain, piece, step, scale_in, w_query, w_key, w_value,
        prompt_keys, prompt_values, cache_keys, cache_values, w_out,
    )


def on_device(
    kv_count,
    tp_count,
    piece_tokens,
    step_tokens,
    in_gain,
    w_query,
    w_key,
    w_value,
    w_out,
    mix_ratio,
    out_gain,
    prompt_keys,
    prompt_values,
    step_cache_keys,
    step_cache_values,
    prompt_len,
    step_lens,
):
    piece_dev = piece_tokens.shape[0]
    step_dev = step_tokens.shape[0]
    heads, maps, dims = w_query.shape[1:]
    wide = w_value.shape[-1]
    mixed, line, key_rows, value_rows = ring_attend(
        step_lens,
        mix_ratio[None, :],
        prompt_len[None, :],
        out_gain[None, :],
        piece_tokens,
        step_tokens,
        in_gain[None, :],
        w_query.reshape(-1, dims),
        w_key.reshape(-1, dims),
        w_value.reshape(-1, wide),
        prompt_keys.reshape(-1, dims),
        prompt_values.reshape(-1, wide),
        step_cache_keys.reshape(-1, dims),
        step_cache_values.reshape(-1, wide),
        w_out.reshape(-1, w_out.shape[-1]),
        kv_count,
        tp_count,
        0,
    )
    piece_out, step_out, piece_k, piece_v, step_k, step_v = finish(mixed, line, key_rows, value_rows)
    return (
        piece_out,
        step_out,
        piece_k.reshape(piece_dev, heads, maps, dims),
        piece_v.reshape(piece_dev, heads, wide),
        step_k.reshape(step_dev, heads, maps, dims),
        step_v.reshape(step_dev, heads, wide),
    )


def solution(mesh):
    in_specs = (
        P("kv", None),
        P("kv", None),
        P(),
        P(None, "tp", None, None),
        P(None, "tp", None, None),
        P(None, "tp", None),
        P("tp", None, None),
        P("tp"),
        P(),
        P("kv", "tp", None, None),
        P("kv", "tp", None),
        P(None, "kv", "tp", None, None),
        P(None, "kv", "tp", None),
        P(),
        P(),
    )
    out_specs = (
        P("kv", "tp"),
        P("kv", "tp"),
        P("kv", "tp", None, None),
        P("kv", "tp", None),
        P("kv", "tp", None, None),
        P("kv", "tp", None),
    )
    return jax.shard_map(
        functools.partial(on_device, mesh.shape["kv"], mesh.shape["tp"]),
        mesh=mesh, in_specs=in_specs, out_specs=out_specs, check_vma=False
    )
```
